32 devices in a mesh: grp: 2 (over y), sp: 4 (over z), dp: 4 (over x, core).
Axes of the slice: x: 2, y: 2, z: 4, core: 2. Of those that a mesh axis runs over, the one named last changes fastest.
Arguments:
- mixer_source_array: bfloat16 [8, 768, 2048], P(('grp', 'dp'), 'sp'), parts along dimension 0, may hold values from -6 to 6
- source_projection: bfloat16 [2048, 1024], P('dp'), may hold values from -0.125 to 0.125
- gating_projection: bfloat16 [2048, 1024], P('dp'), may hold values from -0.125 to 0.125
- entry_mapping_projection: bfloat16 [2048, 256], replicated, may hold values from -0.0390625 to 0.0390625
- readout_mapping_projection: bfloat16 [2048, 256], replicated, may hold values from -0.0390625 to 0.0390625
- increment_projection: bfloat16 [2048, 16], replicated, may hold values from -0.125 to 0.125
- source_conv_taps: float32 [4, 1024], replicated, may hold values from -3 to 3
- entry_mapping_taps: float32 [4, 256], replicated, may hold values from -3 to 3
- readout_mapping_taps: float32 [4, 256], replicated, may hold values from -3 to 3
- increment_offsets: float32 [16], replicated, may hold values from -1 to 1
- channel_damping_rate: float32 [16], replicated, may hold values from 0 to 1
- bypass_coefficients: float32 [16], replicated, may hold values from 0.5 to 1.5
- stride_multiplier: float32 [8, 768], P(('grp', 'dp')), parts along dimension 0, may hold values from 0.5 to 2
- added_log_damping: float32 [8, 768, 16], P(('grp', 'dp')), parts along dimension 0, may hold values from -2.1 to 0
- norm_scale_factor: float32 [1024], replicated, may hold values from 0.1 to 1.9
- final_projection: bfloat16 [1024, 2048], P(None, 'dp'), may hold values from -0.1875 to 0.1875
Outputs:
- output: bfloat16 [8, 768, 2048], P(('grp', 'dp'), 'sp'), parts along dimension 0
The draws below stay inside these ranges and needn't reach their ends.
There are 2 independent parts, one for each index of `grp`. The reference program is written for one: setup_inputs(seed, part) draws one part's arguments, and reference() takes and returns one part's arrays. A program takes and returns all parts, laid end to end along the dimension named above; an argument that names none is the same for every part. Nothing has to cross between parts.
All inputs are finite; a program needn't handle non-finite values.
Results may differ from the reference program's by a relative error of at most 0.015.
Values may be sent and summed in bfloat16 or wider, within the bound.
A program may use at most 64 MiB of HBM per device.

```python
import math
import jax
import jax.numpy as jnp
from jax import lax

D = 2048
H = 16
P_SIZE = 64
N = 128
G = 2
CONV_W = 4
BLK = 64
TOK_DEV = 192
LEN = 768
SEQS = 4


def draw_channel_damping_rate(key, part):
    base = jax.random.fold_in(key, 101)
    key_kind, key_fast, key_slow = jax.random.split(base, 3)
    fast_share = 0.5
    fast_mask = jax.random.uniform(key_kind, (H,), jnp.float32) < fast_share
    fast_rate = jax.random.uniform(key_fast, (H,), jnp.float32, math.log(1.5 / BLK), math.log(2.5 / BLK))
    slow_rate = jax.random.uniform(key_slow, (H,), jnp.float32, math.log(0.1 / LEN), math.log(0.8 / LEN))
    return jnp.exp(jnp.where(fast_mask, fast_rate, slow_rate))


def draw_stride_multiplier(key, part):
    base = jax.random.fold_in(key, 202)
    shards = LEN // TOK_DEV
    factors = jnp.exp(jax.random.uniform(base, (SEQS, shards), jnp.float32, math.log(0.5), math.log(2.0)))
    return jnp.repeat(factors, TOK_DEV, axis=1)


def draw_added_log_damping(key, part):
    base = jax.random.fold_in(key, 303)
    key_spot, key_loss = jax.random.split(base, 2)
    spots = jax.random.randint(key_spot, (SEQS, 3), 0, LEN)
    losses = jax.random.uniform(key_loss, (SEQS, 3, H), jnp.float32, math.log(0.5), math.log(0.8))
    marks = (jnp.arange(LEN)[None, None, :] == spots[:, :, None]).astype(jnp.float32)
    return jnp.einsum('sbl,sbh->slh', marks, losses)


def steps_of(own_key, dims, pieces, least, top_value):
    factor_of, own = 1.0, jax.random.fold_in(own_key, 6)
    for axis_at, shards_of in pieces:
        heights = jnp.exp(jax.random.uniform(jax.random.fold_in(own, axis_at), (shards_of,), jnp.float32, least / len(pieces), top_value / len(pieces)))
        factor_of = factor_of * jnp.repeat(heights, dims[axis_at] // shards_of).reshape([-1 if axis == axis_at else 1 for axis in range(len(dims))])
    return factor_of


def centred(rng, shape, deviation, reach, pieces=(), kind=jnp.bfloat16):
    gain = steps_of(rng, shape, pieces, -0.22, 0.18) if pieces else 1.0
    drawn = jax.random.normal(rng, shape, jnp.float32) * deviation * gain
    return jnp.minimum(jnp.maximum(drawn, -reach), reach).astype(kind)


def setup_inputs(seed: int = 0, part: int = 0) -> dict:
    key_of = jax.random.split(jax.random.key(seed), 17)
    part_keys = jax.random.split(jax.random.fold_in(key_of[16], part), 17)
    return {
        "mixer_source_array": centred(part_keys[0], (SEQS, LEN, D), 1.0, 6.0, ((0, 4), (1, 4))),
        "source_projection": centred(key_of[1], (D, H * P_SIZE), D ** -0.5, 0.125, ((0, 4),)),
        "gating_projection": centred(key_of[2], (D, H * P_SIZE), D ** -0.5, 0.125, ((0, 4),)),
        "entry_mapping_projection": centred(key_of[3], (D, G * N), (10 * D) ** -0.5, 0.0390625),
        "readout_mapping_projection": centred(key_of[4], (D, G * N), (10 * D) ** -0.5, 0.0390625),
        "increment_projection": centred(key_of[5], (D, H), D ** -0.5, 0.125),
        "source_conv_taps": centred(key_of[6], (CONV_W, H * P_SIZE), CONV_W ** -0.5, 3.0, (), jnp.float32),
        "entry_mapping_taps": centred(key_of[7], (CONV_W, G * N), CONV_W ** -0.5, 3.0, (), jnp.float32),
        "readout_mapping_taps": centred(key_of[8], (CONV_W, G * N), CONV_W ** -0.5, 3.0, (), jnp.float32),
        "increment_offsets": jnp.clip(jax.random.uniform(key_of[9], (H,), jnp.float32, -1.0, 1.0), -1.0, 1.0),
        "channel_damping_rate": draw_channel_damping_rate(jax.random.fold_in(key_of[16], 71), part),
        "bypass_coefficients": jnp.clip(jax.random.uniform(key_of[11], (H,), jnp.float32, 0.5, 1.5), 0.5, 1.5),
        "stride_multiplier": draw_stride_multiplier(jax.random.fold_in(jax.random.fold_in(key_of[16], part), 71), part),
        "added_log_damping": draw_added_log_damping(jax.random.fold_in(jax.random.fold_in(key_of[16], part), 71), part),
        "norm_scale_factor": jnp.clip(1.0 + 0.18 * jax.random.normal(key_of[14], (H * P_SIZE,), jnp.float32), 0.1, 1.9),
        "final_projection": centred(key_of[15], (H * P_SIZE, D), (H * P_SIZE) ** -0.5, 0.1875, ((1, 4),)),
    }


EPSILON = 1e-06
HIGH = lax.Precision.HIGHEST

def conv_silu(padded, taps):
    width = taps.shape[0]
    length = padded.shape[0] - width + 1
    total = taps[0][None, :] * padded[0:length]
    for shift_pos in range(1, width):
        total = total + taps[shift_pos][None, :] * padded[shift_pos:shift_pos + length]
    return jax.nn.silu(total).astype(jnp.bfloat16)

def block_parts(x_blocks, b_blocks, c_blocks, step_width_value, logarithm_retain):
    cumulative = jnp.cumsum(logarithm_retain, axis=1)
    scaled = (x_blocks.astype(jnp.float32) * step_width_value[..., None]).astype(jnp.bfloat16)
    intersection = jnp.einsum('kign,kjgn->kgij', c_blocks.astype(jnp.float32), b_blocks.astype(jnp.float32), precision=HIGH)
    by_row = jnp.transpose(cumulative, (0, 2, 3, 1))
    log_gap = by_row[..., :, None] - by_row[..., None, :]
    length = log_gap.shape[-1]
    lower = jnp.tril(jnp.ones((length, length), bool))
    mixing = (intersection[:, :, None] * jnp.exp(jnp.where(lower, log_gap, -jnp.inf))).astype(jnp.bfloat16)
    inner = jnp.einsum('kgrij,kjgrp->kigrp', mixing.astype(jnp.float32), scaled.astype(jnp.float32), precision=HIGH)
    to_end = jnp.exp(cumulative[:, -1:] - cumulative)
    weighted = (b_blocks[:, :, :, None, :].astype(jnp.float32) * to_end[..., None]).astype(jnp.bfloat16)
    states = jnp.einsum('kjgrn,kjgrp->kgrnp', weighted.astype(jnp.float32), scaled.astype(jnp.float32), precision=HIGH)
    return (inner, states, cumulative[:, -1], cumulative)

def block_carry(states, block_total):
    incl_sum = jnp.cumsum(block_total, axis=0)
    excl_sum = incl_sum - block_total
    count = block_total.shape[0]
    log_gap = excl_sum[:, None] - incl_sum[None, :]
    before = (jnp.arange(count)[None, :] < jnp.arange(count)[:, None])[:, :, None, None]
    factors = jnp.exp(jnp.where(before, log_gap, -jnp.inf))
    carried = jnp.einsum('kjgr,jgrnp->kgrnp', factors, states, precision=HIGH)
    return carried

def block_finish(inner, c_blocks, cumulative, carried, x_blocks, skip):
    reached = jnp.einsum('kign,kgrnp->kigrp', c_blocks.astype(jnp.float32), carried, precision=HIGH)
    return inner + reached * jnp.exp(cumulative)[..., None] + skip[..., None] * x_blocks.astype(jnp.float32)

def reference(mixer_source_array, source_projection, gating_projection, entry_mapping_projection, readout_mapping_projection, increment_projection, source_conv_taps, entry_mapping_taps, readout_mapping_taps, increment_offsets, channel_damping_rate, bypass_coefficients, stride_multiplier, added_log_damping, norm_scale_factor, final_projection):
    per_group = H // G
    blocks = LEN // BLK

    def lone_stream_case(input_rows):
        hidden_width, tempo_row_values, surge_row_values = input_rows
        proj_x = jnp.dot(hidden_width, source_projection, preferred_element_type=jnp.float32).astype(jnp.bfloat16)
        gate_z = jnp.dot(hidden_width, gating_projection, preferred_element_type=jnp.float32).astype(jnp.bfloat16)
        proj_b = jnp.dot(hidden_width, entry_mapping_projection, preferred_element_type=jnp.float32).astype(jnp.bfloat16)
        proj_c = jnp.dot(hidden_width, readout_mapping_projection, preferred_element_type=jnp.float32).astype(jnp.bfloat16)
        step_raw = jnp.dot(hidden_width, increment_projection, preferred_element_type=jnp.float32).astype(jnp.bfloat16)
        xs = conv_silu(jnp.concatenate([jnp.zeros((CONV_W - 1, H * P_SIZE), jnp.float32), proj_x.astype(jnp.float32)], 0), source_conv_taps)
        bm = conv_silu(jnp.concatenate([jnp.zeros((CONV_W - 1, G * N), jnp.float32), proj_b.astype(jnp.float32)], 0), entry_mapping_taps)
        cm = conv_silu(jnp.concatenate([jnp.zeros((CONV_W - 1, G * N), jnp.float32), proj_c.astype(jnp.float32)], 0), readout_mapping_taps)
        step_width_value = jax.nn.softplus(step_raw.astype(jnp.float32) + increment_offsets[None, :])
        logarithm_retain = -channel_damping_rate[None, :] * step_width_value * tempo_row_values[:, None] + surge_row_values
        x_blocks = xs.reshape(blocks, BLK, G, per_group, P_SIZE)
        b_blocks = bm.reshape(blocks, BLK, G, N)
        c_blocks = cm.reshape(blocks, BLK, G, N)
        inner, states, block_total, cumulative = block_parts(x_blocks, b_blocks, c_blocks, step_width_value.reshape(blocks, BLK, G, per_group), logarithm_retain.reshape(blocks, BLK, G, per_group))
        carried = block_carry(states, block_total)
        mixed = block_finish(inner, c_blocks, cumulative, carried, x_blocks, bypass_coefficients.reshape(G, per_group))
        mixed = mixed.astype(jnp.bfloat16).reshape(LEN, H * P_SIZE)
        gated = mixed.astype(jnp.float32) * jax.nn.silu(gate_z.astype(jnp.float32))
        grouped = gated.reshape(LEN, G, H * P_SIZE // G)
        normed = grouped * lax.rsqrt(lax.optimization_barrier(jnp.mean(grouped * grouped, axis=-1, keepdims=True)) + EPSILON)
        normed = (normed.reshape(LEN, H * P_SIZE) * norm_scale_factor[None, :]).astype(jnp.bfloat16)
        return jnp.dot(normed, final_projection, preferred_element_type=jnp.float32).astype(jnp.bfloat16)
    return lax.map(lone_stream_case, (mixer_source_array, stride_multiplier, added_log_damping))
```

```python
import functools

import jax
import jax.numpy as jnp
from jax import lax
from jax.experimental import pallas as pl
from jax.experimental.pallas import tpu as pltpu
from jax.sharding import PartitionSpec as P

P_SIZE = 64
N = 128
G = 2
CONV_W = 4
EPSILON = 1e-06
HIGH = lax.Precision.HIGHEST
MESH = pl.DeviceIdType.MESH
HALO = 16
CHUNKS = (128, 256, 128)
TYPES = (2, 2, 4, 4, 3, 4, 3, 4, 2, 4)
X_ORDER = (("S", 0), ("S", 3), ("S", 1), ("S", 2), ("E", 3), ("S", 4), ("E", 2), ("S", 8), ("S", 5), ("S", 6), ("E", 4), ("S", 7), ("E", 5), ("S", 9), ("E", 6), ("E", 9), ("E", 7))
ORDER = (
    ("seeds", 0),
    ("seeds", 3),
    "pbc",
    "nearz",
    ("relay0", 0),
    ("relay1", 0),
    ("seeds", 1),
    ("seeds", 2),
    "nearx",
    ("farx", 3),
    ("state", 3),
    ("relay0", 1),
    ("farx", 0),
    ("relay1", 1),
    ("state", 0),
    ("inner", 3),
    ("seeds", 4),
    ("farx", 2),
    ("state", 2),
    ("farx", 1),
    ("state", 1),
    ("seeds", 8),
    ("inner", 1),
    ("relay0", 4),
    ("inner", 0),
    ("seeds", 5),
    ("relay1", 8),
    ("farz", 4),
    ("relay0", 8),
    ("seeds", 6),
    ("seeds", 7),
    ("inner", 2),
    ("farz", 5),
    ("seeds", 9),
    "finish",
    ("relay0", 6),
    "outn",
    ("out", 8),
    ("out", 9),
    ("out", 7),
    ("out", 6),
)
SLOTS = (
    ((0, 30), (1, 30), (2, 28), (3, 29)),
    ((0, 18), (1, 26), (2, 24), (3, 15)),
    ((0, 24), (1, 29), (2, 27), (3, 22)),
    ((0, 30), (1, 34), (2, 34), (3, 33)),
)


def plan(n_sp, n_x, gw, fw):
    steps = []
    for w, wide in enumerate((gw, gw, fw)):
        cw = min(CHUNKS[w], wide)
        steps += [(w, j, cw) for j in range(wide // cw)]
    if (n_sp, n_x, len(steps)) == (4, 2, len(TYPES)):
        return steps, TYPES, X_ORDER, ORDER, SLOTS
    every = range(len(steps))
    x_order = [(kind, s) for s in every for kind in "SE"]
    order = ["nearz", "pbc", "nearx"]
    for s in every:
        if steps[s][0] == 2 and "outn" not in order:
            order += ["finish", "outn"]
        order += [("seeds", s), ("relay0", s)]
        order += [[("farx", s), ("state", s), ("inner", s)], [("farz", s)], [("out", s)]][steps[s][0]]
    slots = [[(s, order.index("finish")) for s in every if steps[s][0] == 0]] * 4
    return steps, [3] * len(steps), x_order, order, slots
F32 = jnp.float32
BF16 = jnp.bfloat16


def dot(a, b, dims=((1,), (0,)), precision=None):
    return lax.dot_general(a, b, (dims, ((), ())), precision=precision, preferred_element_type=F32)


def silu(v):
    return v * (1.0 / (1.0 + jnp.exp(-v)))


def kernel(
    dims,
    x_hbm,
    wx_hbm,
    wz_hbm,
    wf_hbm,
    wb_hbm,
    wc_hbm,
    wdt_hbm,
    tx_hbm,
    tb_hbm,
    tc_hbm,
    off_hbm,
    rate_hbm,
    skip_hbm,
    stride_hbm,
    damp_hbm,
    scale_hbm,
    out_ref,
    xe,
    wx,
    wz,
    wf,
    wbc,
    wdt,
    tx,
    tb,
    tc,
    off,
    rate,
    skip,
    stride,
    damp,
    scale,
    pbc,
    px,
    pcx,
    gz,
    bm,
    cm,
    cb,
    xs,
    scl,
    sc,
    y,
    st,
    car,
    snd,
    nrm,
    oth,
    loc_sem,
    p_send,
    p_recv,
    link_send,
    seed_recv,
    rest_recv,
    relay_recv,
    c_recv,
    n_recv,
    o_recv,
):
    n_grp, n_sp, n_dp = dims
    n_x = n_dp // 2
    grp, z, dp = (lax.axis_index(a) for a in ("grp", "sp", "dp"))
    xi, core = dp // 2, dp % 2
    tok = out_ref.shape[0]
    heads = off.shape[1]
    per_group = heads // G
    gw = xs.shape[1]
    rows_dev = wx_hbm.shape[0]
    fw = wf_hbm.shape[1]
    width = wf_hbm.shape[0]
    halo_send, x_send, y_send, z_send, c_send, n_send, o_send = (link_send.at[i] for i in range(7))
    halo_recv = p_recv.at[5]
    own_cols = pl.ds(pl.multiple_of(core * gw, 128), gw)
    other_cols = pl.ds(pl.multiple_of((1 - core) * gw, 128), gw)
    partner = {"dp": xi * 2 + 1 - core}
    y_peer = {"grp": 1 - grp}
    zb = z % 2
    z_peer = {"sp": z + 1 - 2 * zb}
    bufs = (wx, wz, wf)
    srcs = (wx_hbm, wz_hbm, wf_hbm)
    own_q = grp * 2 + zb
    y_q = (1 - grp) * 2 + zb
    z_q = grp * 2 + 1 - zb
    far_q = (1 - grp) * 2 + 1 - zb

    barrier = pltpu.get_barrier_semaphore()

    def greet(peer):
        pl.semaphore_signal(barrier, inc=1, device_id=peer, device_id_type=MESH)

    greet(partner)
    greet(y_peer)
    for o in range(1, n_x):
        for d in range(2):
            greet({"dp": lax.rem(xi + o, n_x) * 2 + d})

    @pl.when(z > 0)
    def _():
        for d in range(2):
            greet({"sp": z - 1, "dp": xi * 2 + d})

    @pl.when(z < n_sp - 1)
    def _():
        for d in range(2):
            greet({"sp": z + 1, "dp": xi * 2 + d})

    def remote(src, dst, send, recv, peer):
        return pltpu.make_async_remote_copy(
            src_ref=src, dst_ref=dst, send_sem=send, recv_sem=recv,
            device_id=peer, device_id_type=MESH,
        )

    locals_ = []

    def local(src, dst):
        copy = pltpu.make_async_copy(src, dst, loc_sem.at[len(locals_)])
        copy.start()
        locals_.append(copy)
        return copy

    def far_rows(chip):
        return pl.ds(pl.multiple_of(chip * width, 128), width)

    def seq_rows(s):
        return pl.ds(s * tok, tok)

    dyn_rows = pl.ds(pl.multiple_of(core * tok, 16), tok)
    head_rows = pl.ds(pl.multiple_of(core * per_group, 8), per_group)
    other_heads = pl.ds(pl.multiple_of((1 - core) * per_group, 8), per_group)
    dev_rows = pl.ds(pl.multiple_of(dp * rows_dev, 16), rows_dev)
    partner_rows = pl.ds(pl.multiple_of((xi * 2 + 1 - core) * rows_dev, 16), rows_dev)
    group_n = pl.ds(pl.multiple_of(core * N, 128), N)

    small = [local(x_hbm, xe.at[dyn_rows])]
    small += [local(stride_hbm, stride.at[core]), local(damp_hbm.at[0, head_rows], damp.at[core])]
    small += [local(wdt_hbm, wdt), local(off_hbm, off), local(rate_hbm, rate)]
    maps = [local(wb_hbm.at[:, group_n], wbc.at[:, pl.ds(0, N)])]
    maps += [local(wc_hbm.at[:, group_n], wbc.at[:, pl.ds(N, N)])]
    maps += [local(tb_hbm.at[:, group_n], tb), local(tc_hbm.at[:, group_n], tc)]
    own = [local(srcs[w].at[:, own_cols], bufs[w].at[dev_rows]) for w in range(2)]
    own += [local(wf_hbm, wf.at[far_rows(xi)])]
    late = [local(tx_hbm.at[:, own_cols], tx), local(skip_hbm, skip), local(scale_hbm.at[:, own_cols], scale)]

    greeted = 2 + 2 * (n_x - 1) + 2 * jnp.minimum(z, 1) + 2 * jnp.minimum(n_sp - 1 - z, 1)
    pl.semaphore_wait(barrier, greeted)

    steps, types, x_order, order, slots = plan(n_sp, n_x, gw, fw)
    last_step = len(steps) - 1
    direct, relayed = [], []
    for kind in types:
        turn = sum(1 for d in direct if len(d) == 1) % 2
        direct.append({2: (), 3: (turn,), 4: (0, 1)}[kind])
        relayed.append(tuple(k for k in (0, 1) if k not in direct[-1]))

    def piece_rows(s):
        return width // 8 if steps[s][0] == 2 else rows_dev // 4

    def place(s, chip, q, k):
        w, j, cw = steps[s]
        size = piece_rows(s)
        row = chip * width + (q * 2 + k) * size if w == 2 else (chip * 2 + k) * rows_dev + q * size
        return bufs[w].at[pl.ds(pl.multiple_of(row, 16), size), pl.ds(j * cw, cw)]

    def origin(s, q, k, d):
        w, j, cw = steps[s]
        size = piece_rows(s)
        row, col = ((q * 2 + k) * size, j * cw) if w == 2 else (q * size, d * gw + j * cw)
        return srcs[w].at[pl.ds(pl.multiple_of(row, 16), size), pl.ds(pl.multiple_of(col, 128), cw)]

    def owner_of(o):
        return lax.rem(xi - o + n_x, n_x)

    sent = {"x": [0, 0], "y": 0, "z": 0}

    def x_start(s, o, q, k, d, recv):
        peer = {"dp": lax.rem(xi + o, n_x) * 2 + d}
        remote(origin(s, q, k, d), place(s, xi, q, k), x_send, recv.at[s], peer).start()

    def unit(s):
        return piece_rows(s) * steps[s][2] // gw

    def x_seeds(s):
        for o in range(1, n_x):
            if steps[s][0] == 2:
                for k in range(2):
                    x_start(s, o, own_q, k, core, seed_recv)
            else:
                for d in (core, 1 - core):
                    x_start(s, o, own_q, core, d, seed_recv)
            for k in range(2):
                sent["x"][k] += 2 * unit(s)

    def x_extras(s):
        for o in range(1, n_x):
            if steps[s][0] == 2:
                for k in direct[s]:
                    x_start(s, o, far_q, k, core, rest_recv)
                    sent["x"][0] += unit(s)
                    sent["x"][1] += unit(s)
            elif len(direct[s]) == 2:
                for d in (core, 1 - core):
                    x_start(s, o, far_q, core, d, rest_recv)
                sent["x"][0] += 2 * unit(s)
                sent["x"][1] += 2 * unit(s)
            else:
                for k in direct[s]:
                    sent["x"][k] += 2 * unit(s)

                    @pl.when(core == k)
                    def _(k=k, o=o):
                        for d in (core, 1 - core):
                            x_start(s, o, far_q, k, d, rest_recv)

    def y_start(s, o, q, k):
        spot = place(s, owner_of(o), q, k)
        remote(spot, spot, y_send, rest_recv.at[s], y_peer).start()
        sent["y"] += unit(s)

    def z_start(s, o, k):
        spot = place(s, owner_of(o), own_q, k)
        recv = relay_recv.at[s, k] if k in relayed[s] else rest_recv.at[s]
        remote(spot, spot, z_send, recv, z_peer).start()
        sent["z"] += unit(s)

    def pieces_wait(s, count, recv):
        w, j, cw = steps[s]
        spot = bufs[w].at[pl.ds(0, count * (n_x - 1) * piece_rows(s)), pl.ds(j * cw, cw)]
        remote(spot, spot, x_send, recv, partner).wait_recv()

    def halo_copies():
        up = jnp.minimum(z + 1, n_sp - 1)
        dst = xe.at[pl.ds(pl.multiple_of(2 * tok + core * HALO, 16), HALO)]
        src = x_hbm.at[pl.ds(tok - HALO, HALO)]
        return [remote(src, dst, halo_send, halo_recv, {"sp": up, "dp": xi * 2 + d}) for d in (core, 1 - core)]

    @pl.when(z < n_sp - 1)
    def _():
        for copy in halo_copies():
            copy.start()

    sends = []

    def start(copy):
        copy.start()
        sends.append(copy)

    for n, (kind, s) in enumerate(x_order):
        (x_seeds if kind == "S" else x_extras)(s)
        if n == 0:
            start(remote(x_hbm, xe.at[dyn_rows], p_send.at[0], p_recv.at[0], partner))
            start(remote(stride_hbm, stride.at[core], p_send.at[1], p_recv.at[1], partner))
            start(remote(damp_hbm.at[0, other_heads], damp.at[core], p_send.at[2], p_recv.at[2], partner))
            for w in range(2):
                start(remote(srcs[w].at[:, other_cols], bufs[w].at[dev_rows], p_send.at[3 + w], p_recv.at[3 + w], partner))

    def seeds(s):
        pieces_wait(s, 2, seed_recv.at[s])
        for o in range(1, n_x):
            for k in relayed[s] + direct[s]:
                z_start(s, o, k)
            for k in range(2):
                y_start(s, o, own_q, k)

    def relay(s, r):
        k = relayed[s][r]
        pieces_wait(s, 1, relay_recv.at[s, k])
        for o in range(1, n_x):
            y_start(s, o, z_q, k)

    def rest(s):
        pieces_wait(s, 6 - len(relayed[s]), rest_recv.at[s])

    depth = 2 * rows_dev

    def chip_rows(o):
        return pl.ds(pl.multiple_of(owner_of(o) * depth, 128), depth)

    def square_iota(size):
        return [lax.broadcasted_iota(jnp.int32, (size, size), d) for d in (0, 1)]

    def pick(values, axis):
        low, high = (lax.slice_in_dim(values, i * per_group, (i + 1) * per_group, axis=axis) for i in range(2))
        return jnp.where(core == 0, low, high)

    def column(ref):
        i, j = square_iota(heads)
        mine = pick(jnp.sum(jnp.where(i == j, ref[...], 0.0), axis=1, keepdims=True), 0)
        return jnp.concatenate([mine, mine], axis=0)

    def my_positions(values):
        mine = values[:, 0:tok]
        for i in range(1, n_sp):
            mine = jnp.where(z == i, values[:, i * tok : (i + 1) * tok], mine)
        return mine

    for copy in small:
        copy.wait()
    other_seq = xe.at[pl.ds(pl.multiple_of((1 - core) * tok, 16), tok)]
    remote(x_hbm, other_seq, p_send.at[0], p_recv.at[0], partner).wait_recv()
    remote(stride_hbm, stride.at[1 - core], p_send.at[1], p_recv.at[1], partner).wait_recv()
    remote(damp_hbm.at[0, other_heads], damp.at[1 - core], p_send.at[2], p_recv.at[2], partner).wait_recv()

    raw = [pick(dot(wdt[...], xe[seq_rows(s), :], ((1,), (1,))), 0) for s in range(2)]
    raw = jnp.concatenate(raw, axis=0).astype(BF16).astype(F32)
    pre = raw + column(off)
    step_t = jnp.maximum(pre, 0.0) + jnp.log1p(jnp.exp(-jnp.abs(pre)))
    tempo = [jnp.broadcast_to(my_positions(stride[s]), (per_group, tok)) for s in range(2)]
    extra = [my_positions(damp[s]) for s in range(2)]
    keep = -column(rate) * step_t * jnp.concatenate(tempo, axis=0) + jnp.concatenate(extra, axis=0)
    row, col = square_iota(tok)
    lower = row >= col
    step = dot((row == col).astype(F32), step_t, ((1,), (1,)), HIGH)
    cum = dot(lower.astype(F32), keep, ((1,), (1,)), HIGH)
    cum_t = dot(keep, (row <= col).astype(F32), precision=HIGH)
    last = cum[tok - 1 : tok, :]
    to_end = jnp.exp(last - cum)
    reach = jnp.exp(cum)
    whole = jnp.exp(last)
    first_head = lax.broadcasted_iota(jnp.int32, (tok, 2 * P_SIZE), 1) < P_SIZE
    first_row = first_head[0:1, :]

    def spread(values, p, mask):
        return jnp.where(mask, values[:, 2 * p : 2 * p + 1], values[:, 2 * p + 1 : 2 * p + 2])

    def pair_cols(p):
        return pl.ds(p * 2 * P_SIZE, 2 * P_SIZE)

    pairs = per_group // 2
    main = pl.ds(0, 2 * tok)
    span = HALO + tok

    def near(w):
        own[w].wait()
        spot = bufs[w].at[partner_rows]
        remote(spot, spot, p_send.at[3 + w], p_recv.at[3 + w], partner).wait_recv()

    def tiles(width, tile, body):
        def run(j, carry):
            body(pl.ds(pl.multiple_of(j * tile, tile), tile))
            return carry

        lax.fori_loop(0, width // tile, run, 0)

    def near_z(cols):
        gz[:, cols] = dot(xe[main, chip_rows(0)], wz[chip_rows(0), cols])

    def put(buf, cols, values):
        for s in range(2):
            buf[pl.ds(s * span, HALO), cols] = values[2 * tok + s * HALO : 2 * tok + (s + 1) * HALO, :]
            buf[pl.ds(s * span + HALO, tok), cols] = values[s * tok : (s + 1) * tok, :]

    def conv(buf, s, cols, taps):
        first = s * span + HALO - CONV_W + 1
        total = taps[0:1, :] * buf[pl.ds(first, tok), cols]
        for k in range(1, CONV_W):
            total = total + taps[k : k + 1, :] * buf[pl.ds(first + k, tok), cols]
        return silu(total).astype(BF16)

    skip_vals = []

    def near_x(cols):
        px[:, cols] = dot(xe[:, chip_rows(0)], wx[chip_rows(0), cols])

    def maps_task():
        @pl.when(z == 0)
        def _():
            xe[pl.ds(2 * tok, 2 * HALO), :] = jnp.zeros((2 * HALO, xe.shape[1]), BF16)

        @pl.when(z > 0)
        def _():
            spot = xe.at[pl.ds(2 * tok, 2 * HALO)]
            remote(spot, spot, halo_send, halo_recv, partner).wait_recv()

        for copy in maps:
            copy.wait()
        put(pbc, pl.ds(0, 2 * N), dot(xe[...], wbc[...]).astype(BF16).astype(F32))
        for s in range(2):
            bm[seq_rows(s), :] = conv(pbc, s, pl.ds(0, N), tb[...])
            cm[seq_rows(s), :] = conv(pbc, s, pl.ds(N, N), tc[...])
        for s in range(2):
            cb[s] = dot(cm[seq_rows(s), :], bm[seq_rows(s), :], ((1,), (1,)))
        for copy in late:
            copy.wait()
        skip_vals.append(pick(skip[...], 1))

    def far_x(cols):
        acc = px[:, cols]
        for o in range(1, n_x):
            acc = acc + dot(xe[:, chip_rows(o)], wx[chip_rows(o), cols])
        put(pcx, cols, acc.astype(BF16).astype(F32))
        for s in range(2):
            xs[seq_rows(s), cols] = conv(pcx, s, cols, tx[:, cols])

    def far_z(cols):
        acc = gz[:, cols]
        for o in range(1, n_x):
            acc = acc + dot(xe[main, chip_rows(o)], wz[chip_rows(o), cols])
        gz[:, cols] = silu(acc.astype(BF16).astype(F32))

    def chain_copy(s, p):
        pc = pair_cols(p)
        return remote(
            snd.at[s, :, pc], car.at[s, :, pc], c_send, c_recv.at[s, p],
            {"sp": jnp.minimum(z + 1, n_sp - 1)},
        )

    def step_pairs(cols):
        return range(cols.start // (2 * P_SIZE), (cols.start + cols.size) // (2 * P_SIZE))

    def local_state(cols):
        for s in range(2):
            for p in step_pairs(cols):
                pc = pair_cols(p)
                v = s * pairs + p
                part = (xs[seq_rows(s), pc].astype(F32) * spread(step, v, first_head)).astype(BF16)
                scl[seq_rows(s), pc] = part
                sc[seq_rows(s), pc] = (part.astype(F32) * spread(to_end, v, first_head)).astype(BF16)
            st[s, :, cols] = dot(bm[seq_rows(s), :], sc[seq_rows(s), cols], ((0,), (0,)))

        @pl.when(z == 0)
        def _():
            for s in range(2):
                car[s, :, cols] = jnp.zeros((N, cols.size), BF16)
                for p in step_pairs(cols):
                    pc = pair_cols(p)
                    snd[s, :, pc] = st[s, :, pc].astype(BF16)
                    chain_copy(s, p).start()

    def chain(cols):
        for s in range(2):
            for p in step_pairs(cols):
                chain_copy(s, p).wait_recv()

                @pl.when(z < n_sp - 1)
                def _(s=s, p=p):
                    pc = pair_cols(p)
                    v = s * pairs + p
                    total = spread(whole, v, first_row) * car[s, :, pc].astype(F32) + st[s, :, pc]
                    snd[s, :, pc] = total.astype(BF16)
                    chain_copy(s, p).start()

    def chain_slot(slot, cols):
        @pl.when(jnp.minimum(z, 3) == slot)
        def _():
            chain(cols)

    def inner(s, cols):
        for p in step_pairs(cols):
            pc = pair_cols(p)
            parts = []
            for v in (s * per_group + 2 * p, s * per_group + 2 * p + 1):
                gap = jnp.where(lower, cum[:, v : v + 1] - cum_t[v : v + 1, :], -jnp.inf)
                parts.append(dot((cb[s] * jnp.exp(gap)).astype(BF16), scl[seq_rows(s), pc]))
            bypass = spread(skip_vals[0], p, first_row) * xs[seq_rows(s), pc].astype(F32)
            y[seq_rows(s), pc] = jnp.where(first_head, parts[0], parts[1]) + bypass

    def step_cols(s):
        return pl.ds(steps[s][1] * steps[s][2], steps[s][2])

    def slot_rows(s, swap):
        return pl.ds(pl.multiple_of(lax.rem(s + core + swap, 2) * tok, 16), tok)

    def finish(s):
        reached = dot(cm[seq_rows(s), :], car[s])
        square = jnp.zeros((tok, 1), F32)
        for p in range(pairs):
            pc = pair_cols(p)
            here = slice(p * 2 * P_SIZE, (p + 1) * 2 * P_SIZE)
            mixed = y[seq_rows(s), pc] + spread(reach, s * pairs + p, first_head) * reached[:, here]
            gated = mixed.astype(BF16).astype(F32) * gz[seq_rows(s), pc]
            square = square + jnp.sum(gated * gated, axis=1, keepdims=True)
            y[seq_rows(s), pc] = gated
        inv = lax.rsqrt(square * (1.0 / gw) + EPSILON)
        nrm[slot_rows(s, 0), own_cols] = (y[seq_rows(s), :] * inv * scale[...]).astype(BF16)
        remote(
            nrm.at[slot_rows(s, 0), own_cols], nrm.at[slot_rows(s, 1), own_cols],
            n_send, n_recv.at[0], partner,
        ).start()

    def out_cols(o, s, d):
        cols = step_cols(s)
        return pl.ds(pl.multiple_of((owner_of(o) * 2 + d) * fw + cols.start, 128), cols.size)

    def out_copy(o, s, d):
        cols = step_cols(s)
        return remote(
            oth.at[:, pl.ds(o * fw + cols.start, cols.size)], out_ref.at[:, out_cols(o, s, d)],
            o_send, o_recv.at[0], partner,
        )

    def output(o, s):
        cols = step_cols(s)
        part = dot(nrm[...], wf[far_rows(owner_of(o)), cols]).astype(BF16)
        out_ref[:, out_cols(o, s, core)] = part[0:tok, :]
        oth[:, pl.ds(o * fw + cols.start, cols.size)] = part[tok : 2 * tok, :]
        out_copy(o, s, core).start()

    f_steps = [s for s in range(len(steps)) if steps[s][0] == 2]

    def out_near():
        own[2].wait()
        spot = nrm.at[:, other_cols]
        remote(spot, spot, n_send, n_recv.at[0], partner).wait_recv()
        for s in f_steps:
            output(0, s)

    def run(name):
        if name == "nearz":
            near(1)
            tiles(gw, 256, near_z)
        elif name == "pbc":
            maps_task()
        elif name == "nearx":
            near(0)
            tiles(gw, 256, near_x)
        elif name == "finish":
            for s in range(2):
                finish(s)
        elif name == "outn":
            out_near()
        else:
            task, s = name
            cols = step_cols(s)
            if task == "seeds":
                seeds(s)
            elif task in ("relay0", "relay1"):
                relay(s, int(task[-1]))
            elif task == "farx":
                rest(s)
                far_x(cols)
            elif task == "state":
                local_state(cols)
            elif task == "inner":
                for q in range(2):
                    inner(q, cols)
            elif task == "farz":
                rest(s)
                far_z(cols)
            else:
                rest(s)
                for o in range(1, n_x):
                    output(o, s)

    for n, name in enumerate(order):
        for level in (1, 2, 3):
            for s, at in slots[level]:
                if at == n:
                    chain_slot(level, step_cols(s))
        run(name)
    remote(oth, oth, o_send, o_recv.at[0], partner).wait_recv()

    def sent_wait(send, rows):
        if rows:
            spot = wx.at[pl.ds(0, rows)]
            remote(spot, spot, send, n_recv.at[0], partner).wait_send()

    for copy in sends:
        copy.wait_send()
    sent_wait(y_send, sent["y"])
    sent_wait(z_send, sent["z"])
    if sent["x"][0] == sent["x"][1]:
        sent_wait(x_send, sent["x"][0])
    else:
        for k in range(2):

            @pl.when(core == k)
            def _(k=k):
                sent_wait(x_send, sent["x"][k])

    spot = nrm.at[:, own_cols]
    remote(spot, spot, n_send, n_recv.at[0], partner).wait_send()
    remote(oth, oth, o_send, o_recv.at[0], partner).wait_send()

    @pl.when(z < n_sp - 1)
    def _():
        spot = xe.at[pl.ds(2 * tok, 2 * HALO)]
        remote(spot, spot, halo_send, halo_recv, partner).wait_send()
        remote(snd, snd, c_send, n_recv.at[0], partner).wait_send()


def shards(
    dims,
    mixer_source_array,
    source_projection,
    gating_projection,
    entry_mapping_projection,
    readout_mapping_projection,
    increment_projection,
    source_conv_taps,
    entry_mapping_taps,
    readout_mapping_taps,
    increment_offsets,
    channel_damping_rate,
    bypass_coefficients,
    stride_multiplier,
    added_log_damping,
    norm_scale_factor,
    final_projection,
):
    n_grp, n_sp, n_dp = dims
    n_x = n_dp // 2
    hidden = mixer_source_array[0]
    tok, model = hidden.shape
    width = source_projection.shape[1]
    gw = width // G
    heads = increment_projection.shape[1]
    fw = final_projection.shape[1]
    length = stride_multiplier.shape[1]
    out_width = fw * n_dp
    n_steps = len(plan(n_sp, n_x, gw, fw)[0])
    span = HALO + tok
    dma = pltpu.SemaphoreType.DMA
    hbm = pl.BlockSpec(memory_space=pl.ANY)
    output = pl.pallas_call(
        functools.partial(kernel, dims),
        out_shape=pltpu.VMEM((tok, out_width), BF16),
        in_specs=[hbm] * 16,
        out_specs=pl.BlockSpec(memory_space=pltpu.VMEM),
        scratch_shapes=[
            pltpu.VMEM((2 * span, model), BF16),
            pltpu.VMEM((model, gw), BF16),
            pltpu.VMEM((model, gw), BF16),
            pltpu.VMEM((n_x * width, fw), BF16),
            pltpu.VMEM((model, 2 * N), BF16),
            pltpu.VMEM((heads, model), BF16),
            pltpu.VMEM((CONV_W, gw), F32),
            pltpu.VMEM((CONV_W, N), F32),
            pltpu.VMEM((CONV_W, N), F32),
            pltpu.VMEM((1, heads), F32),
            pltpu.VMEM((1, heads), F32),
            pltpu.VMEM((1, heads), F32),
            pltpu.VMEM((2, 1, length), F32),
            pltpu.VMEM((2, heads // G, length), F32),
            pltpu.VMEM((1, gw), F32),
            pltpu.VMEM((2 * span, 2 * N), F32),
            pltpu.VMEM((2 * span, gw), F32),
            pltpu.VMEM((2 * span, gw), F32),
            pltpu.VMEM((2 * tok, gw), F32),
            pltpu.VMEM((2 * tok, N), BF16),
            pltpu.VMEM((2 * tok, N), BF16),
            pltpu.VMEM((2, tok, tok), F32),
            pltpu.VMEM((2 * tok, gw), BF16),
            pltpu.VMEM((2 * tok, gw), BF16),
            pltpu.VMEM((2 * tok, gw), BF16),
            pltpu.VMEM((2 * tok, gw), F32),
            pltpu.VMEM((2, N, gw), F32),
            pltpu.VMEM((2, N, gw), BF16),
            pltpu.VMEM((2, N, gw), BF16),
            pltpu.VMEM((2 * tok, width), BF16),
            pltpu.VMEM((tok, n_x * fw), BF16),
            dma((16,)),
            dma((5,)),
            dma((6,)),
            dma((7,)),
            dma((n_steps,)),
            dma((n_steps,)),
            dma((n_steps, 2)),
            dma((2, heads // G // 2)),
            dma((1,)),
            dma((1,)),
        ],
        compiler_params=pltpu.CompilerParams(
            collective_id=0, has_side_effects=True, vmem_limit_bytes=56 * 1024 * 1024
        ),
    )(
        hidden,
        source_projection,
        gating_projection,
        final_projection,
        entry_mapping_projection,
        readout_mapping_projection,
        increment_projection.T,
        source_conv_taps,
        entry_mapping_taps,
        readout_mapping_taps,
        increment_offsets[None],
        channel_damping_rate[None],
        bypass_coefficients[None],
        stride_multiplier,
        jnp.swapaxes(added_log_damping, 1, 2),
        norm_scale_factor[None],
    )
    return output[None]


def solution(mesh):
    n_grp, n_sp, n_dp = (mesh.shape[a] for a in ("grp", "sp", "dp"))
    return jax.shard_map(
        functools.partial(shards, (n_grp, n_sp, n_dp)),
        mesh=mesh,
        in_specs=(
            P(("grp", "dp"), "sp", None),
            P("dp", None),
            P("dp", None),
            P(),
            P(),
            P(),
            P(),
            P(),
            P(),
            P(),
            P(),
            P(),
            P(("grp", "dp"), None),
            P(("grp", "dp"), None, None),
            P(),
            P(None, "dp"),
        ),
        out_specs=P(("grp", "dp"), "sp", None),
        check_vma=False,
    )
```

```python
import functools

import jax
import jax.numpy as jnp
from jax import lax
from jax.experimental import pallas as pl
from jax.experimental.pallas import tpu as pltpu
from jax.sharding import PartitionSpec as P

P_SIZE = 64
N = 128
G = 2
CONV_W = 4
EPSILON = 1e-06
HIGH = lax.Precision.HIGHEST
MESH = pl.DeviceIdType.MESH
HALO = 16
CHUNKS = (128, 256, 128)
TYPES = (2, 2, 4, 4, 3, 4, 3, 4, 2, 4)
X_ORDER = (("S", 3), ("S", 0), ("S", 1), ("S", 2), ("E", 3), ("S", 4), ("S", 8), ("E", 2), ("S", 5), ("S", 7), ("S", 6), ("E", 5), ("S", 9), ("E", 4), ("E", 7), ("E", 6), ("E", 9))
ORDER = (
    ("seeds", 3),
    ("seeds", 0),
    ("seeds", 1),
    "pbc",
    ("seeds", 2),
    "nearx",
    ("relay1", 0),
    ("relay0", 0),
    "nearz",
    ("farx", 3),
    ("relay0", 1),
    ("state", 3),
    ("relay1", 1),
    ("seeds", 4),
    ("farx", 0),
    ("state", 0),
    ("seeds", 8),
    ("farx", 2),
    ("state", 2),
    ("farx", 1),
    ("state", 1),
    ("relay0", 4),
    ("seeds", 5),
    ("relay1", 8),
    ("relay0", 8),
    ("inner", 3),
    ("seeds", 6),
    ("inner", 0),
    ("seeds", 7),
    ("inner", 2),
    ("fwd", 8),
    ("farz", 5),
    ("relay0", 6),
    ("seeds", 9),
    ("farz", 4),
    ("inner", 1),
    "finishp",
    "finisho",
    ("fwd", 7),
    ("fwd", 6),
    "outa",
    "outb",
    ("fwd", 9),
    ("out", 8),
    ("out", 7),
    ("out", 6),
    ("out", 9),
)
SLOTS = (
    ((0, 21), (1, 33), (2, 23), (3, 21)),
    ((0, 22), (1, 28), (2, 26), (3, 15)),
    ((0, 23), (1, 28), (2, 27), (3, 20)),
    ((0, 30), (1, 36), (2, 36), (3, 29)),
)
F32 = jnp.float32
BF16 = jnp.bfloat16


def plan(n_sp, n_x, gw, fw):
    steps = []
    for w, wide in enumerate((gw, gw, fw)):
        cw = min(CHUNKS[w], wide)
        steps += [(w, j, cw) for j in range(wide // cw)]
    if (n_sp, n_x, len(steps)) == (4, 2, len(TYPES)):
        return steps, TYPES, X_ORDER, ORDER, SLOTS
    every = range(len(steps))
    x_order = [(kind, s) for s in every for kind in "SE"]
    order = ["nearz", "pbc", "nearx"]
    for s in every:
        order += [("seeds", s), ("relay0", s)]
        order += [[("farx", s), ("state", s), ("inner", s)], [("farz", s)], [("fwd", s)]][steps[s][0]]
    order += ["finishp", "finisho", "outa", "outb"]
    order += [("out", s) for s in every if steps[s][0] == 2]
    slots = [[(s, order.index("finishp")) for s in every if steps[s][0] == 0]] * 4
    return steps, [3] * len(steps), x_order, order, slots


def dot(a, b, dims=((1,), (0,)), precision=None):
    return lax.dot_general(a, b, (dims, ((), ())), precision=precision, preferred_element_type=F32)


def silu(v):
    return v * (1.0 / (1.0 + jnp.exp(-v)))


def kernel(
    dims,
    x_hbm,
    wx_hbm,
    wz_hbm,
    wf_hbm,
    wb_hbm,
    wc_hbm,
    wdt_hbm,
    tx_hbm,
    tb_hbm,
    tc_hbm,
    off_hbm,
    rate_hbm,
    skip_hbm,
    stride_hbm,
    damp_hbm,
    scale_hbm,
    out_ref,
    xe,
    wx,
    wz,
    wf,
    wbc,
    wdt,
    tx,
    tb,
    tc,
    off,
    rate,
    skip,
    stride,
    damp,
    scale,
    pbc,
    px,
    pcx,
    gz,
    bm,
    cm,
    cb,
    xs,
    scl,
    sc,
    y,
    st,
    car,
    snd,
    nrm,
    nsn,
    acc,
    loc_sem,
    p_send,
    p_recv,
    link_send,
    seed_recv,
    rest_recv,
    relay_recv,
    c_recv,
    n_recv,
    f_recv,
):
    n_grp, n_sp, n_dp = dims
    n_x = n_dp // 2
    grp, z, dp = (lax.axis_index(a) for a in ("grp", "sp", "dp"))
    xi, core = dp // 2, dp % 2
    tok = out_ref.shape[0]
    heads = off.shape[1]
    per_group = heads // G
    gw = xs.shape[1]
    rows_dev = wx_hbm.shape[0]
    fw = wf_hbm.shape[1]
    width = wf_hbm.shape[0]
    halo_send, x_send, y_send, z_send, c_send, n_send, f_send = (link_send.at[i] for i in range(7))
    halo_recv = p_recv.at[6]
    own_cols = pl.ds(pl.multiple_of(core * gw, 128), gw)
    other_cols = pl.ds(pl.multiple_of((1 - core) * gw, 128), gw)
    partner = {"dp": xi * 2 + 1 - core}
    y_peer = {"grp": 1 - grp}
    zb = z % 2
    z_peer = {"sp": z + 1 - 2 * zb}
    bufs = (wx, wz, wf)
    srcs = (wx_hbm, wz_hbm, wf_hbm)
    own_q = grp * 2 + zb
    y_q = (1 - grp) * 2 + zb
    z_q = grp * 2 + 1 - zb
    far_q = (1 - grp) * 2 + 1 - zb

    barrier = pltpu.get_barrier_semaphore()

    def greet(peer):
        pl.semaphore_signal(barrier, inc=1, device_id=peer, device_id_type=MESH)

    greet(partner)
    greet(y_peer)
    for o in range(1, n_x):
        for d in range(2):
            greet({"dp": lax.rem(xi + o, n_x) * 2 + d})

    @pl.when(z > 0)
    def _():
        for d in range(2):
            greet({"sp": z - 1, "dp": xi * 2 + d})

    @pl.when(z < n_sp - 1)
    def _():
        for d in range(2):
            greet({"sp": z + 1, "dp": xi * 2 + d})

    def remote(src, dst, send, recv, peer):
        return pltpu.make_async_remote_copy(
            src_ref=src, dst_ref=dst, send_sem=send, recv_sem=recv,
            device_id=peer, device_id_type=MESH,
        )

    locals_ = []

    def local(src, dst):
        copy = pltpu.make_async_copy(src, dst, loc_sem.at[len(locals_)])
        copy.start()
        locals_.append(copy)
        return copy

    def out_rows(d):
        return pl.ds(pl.multiple_of(d * width, 128), width)

    def seq_rows(s):
        return pl.ds(s * tok, tok)

    dyn_rows = pl.ds(pl.multiple_of(core * tok, 16), tok)
    head_rows = pl.ds(pl.multiple_of(core * per_group, 8), per_group)
    other_heads = pl.ds(pl.multiple_of((1 - core) * per_group, 8), per_group)
    dev_rows = pl.ds(pl.multiple_of(dp * rows_dev, 16), rows_dev)
    partner_rows = pl.ds(pl.multiple_of((xi * 2 + 1 - core) * rows_dev, 16), rows_dev)
    group_n = pl.ds(pl.multiple_of(core * N, 128), N)

    small = [local(x_hbm, xe.at[dyn_rows])]
    small += [local(stride_hbm, stride.at[core]), local(damp_hbm.at[0, head_rows], damp.at[core])]
    small += [local(wdt_hbm, wdt), local(off_hbm, off), local(rate_hbm, rate)]
    maps = [local(wb_hbm.at[:, group_n], wbc.at[:, pl.ds(0, N)])]
    maps += [local(wc_hbm.at[:, group_n], wbc.at[:, pl.ds(N, N)])]
    maps += [local(tb_hbm.at[:, group_n], tb), local(tc_hbm.at[:, group_n], tc)]
    own = [local(srcs[w].at[:, own_cols], bufs[w].at[dev_rows]) for w in range(2)]
    own += [local(wf_hbm, wf.at[out_rows(dp)])]
    late = [local(tx_hbm.at[:, own_cols], tx), local(skip_hbm, skip), local(scale_hbm.at[:, own_cols], scale)]

    greeted = 2 + 2 * (n_x - 1) + 2 * jnp.minimum(z, 1) + 2 * jnp.minimum(n_sp - 1 - z, 1)
    pl.semaphore_wait(barrier, greeted)

    steps, types, x_order, order, slots = plan(n_sp, n_x, gw, fw)
    last_step = len(steps) - 1
    direct, relayed = [], []
    for kind in types:
        turn = sum(1 for d in direct if len(d) == 1) % 2
        direct.append({2: (), 3: (turn,), 4: (0, 1)}[kind])
        relayed.append(tuple(k for k in (0, 1) if k not in direct[-1]))

    def piece_rows(s):
        return width // 8 if steps[s][0] == 2 else rows_dev // 4

    def place(s, chip, q, k):
        w, j, cw = steps[s]
        size = piece_rows(s)
        row = (chip * 2 + core) * width + (q * 2 + k) * size if w == 2 else (chip * 2 + k) * rows_dev + q * size
        return bufs[w].at[pl.ds(pl.multiple_of(row, 16), size), pl.ds(j * cw, cw)]

    def origin(s, q, k, d):
        w, j, cw = steps[s]
        size = piece_rows(s)
        row, col = ((q * 2 + k) * size, j * cw) if w == 2 else (q * size, d * gw + j * cw)
        return srcs[w].at[pl.ds(pl.multiple_of(row, 16), size), pl.ds(pl.multiple_of(col, 128), cw)]

    def owner_of(o):
        return lax.rem(xi - o + n_x, n_x)

    sent = {"x": [0, 0], "y": 0, "z": 0}

    def x_start(s, o, q, k, d, recv):
        peer = {"dp": lax.rem(xi + o, n_x) * 2 + d}
        remote(origin(s, q, k, d), place(s, xi, q, k), x_send, recv.at[s], peer).start()

    def unit(s):
        return piece_rows(s) * steps[s][2] // gw

    def x_seeds(s):
        for o in range(1, n_x):
            if steps[s][0] == 2:
                for k in range(2):
                    x_start(s, o, own_q, k, core, seed_recv)
            else:
                for d in (core, 1 - core):
                    x_start(s, o, own_q, core, d, seed_recv)
            for k in range(2):
                sent["x"][k] += 2 * unit(s)

    def x_extras(s):
        for o in range(1, n_x):
            if steps[s][0] == 2:
                for k in direct[s]:
                    x_start(s, o, far_q, k, core, rest_recv)
                    sent["x"][0] += unit(s)
                    sent["x"][1] += unit(s)
            elif len(direct[s]) == 2:
                for d in (core, 1 - core):
                    x_start(s, o, far_q, core, d, rest_recv)
                sent["x"][0] += 2 * unit(s)
                sent["x"][1] += 2 * unit(s)
            else:
                for k in direct[s]:
                    sent["x"][k] += 2 * unit(s)

                    @pl.when(core == k)
                    def _(k=k, o=o):
                        for d in (core, 1 - core):
                            x_start(s, o, far_q, k, d, rest_recv)

    def y_start(s, o, q, k):
        spot = place(s, owner_of(o), q, k)
        remote(spot, spot, y_send, rest_recv.at[s], y_peer).start()
        sent["y"] += unit(s)

    def z_start(s, o, k):
        spot = place(s, owner_of(o), own_q, k)
        recv = relay_recv.at[s, k] if k in relayed[s] else rest_recv.at[s]
        remote(spot, spot, z_send, recv, z_peer).start()
        sent["z"] += unit(s)

    def pieces_wait(s, count, recv):
        w, j, cw = steps[s]
        spot = bufs[w].at[pl.ds(0, count * (n_x - 1) * piece_rows(s)), pl.ds(j * cw, cw)]
        remote(spot, spot, x_send, recv, partner).wait_recv()

    def halo_copies():
        up = jnp.minimum(z + 1, n_sp - 1)
        dst = xe.at[pl.ds(pl.multiple_of(2 * tok + core * HALO, 16), HALO)]
        src = x_hbm.at[pl.ds(tok - HALO, HALO)]
        return [remote(src, dst, halo_send, halo_recv, {"sp": up, "dp": xi * 2 + d}) for d in (core, 1 - core)]

    @pl.when(z < n_sp - 1)
    def _():
        for copy in halo_copies():
            copy.start()

    sends = []

    def start(copy):
        copy.start()
        sends.append(copy)

    for n, (kind, s) in enumerate(x_order):
        (x_seeds if kind == "S" else x_extras)(s)
        if n == 0:
            start(remote(x_hbm, xe.at[dyn_rows], p_send.at[0], p_recv.at[0], partner))
            start(remote(stride_hbm, stride.at[core], p_send.at[1], p_recv.at[1], partner))
            start(remote(damp_hbm.at[0, other_heads], damp.at[core], p_send.at[2], p_recv.at[2], partner))
            for w in range(2):
                start(remote(srcs[w].at[:, other_cols], bufs[w].at[dev_rows], p_send.at[3 + w], p_recv.at[3 + w], partner))
            start(remote(wf_hbm, wf.at[out_rows(dp)], p_send.at[5], p_recv.at[5], partner))

    def seeds(s):
        pieces_wait(s, 2, seed_recv.at[s])
        for o in range(1, n_x):
            for k in relayed[s] + direct[s]:
                z_start(s, o, k)
            for k in range(2):
                y_start(s, o, own_q, k)

    def relay(s, r):
        k = relayed[s][r]
        pieces_wait(s, 1, relay_recv.at[s, k])
        for o in range(1, n_x):
            y_start(s, o, z_q, k)

    def rest(s):
        pieces_wait(s, 6 - len(relayed[s]), rest_recv.at[s])

    depth = 2 * rows_dev

    def chip_rows(o):
        return pl.ds(pl.multiple_of(owner_of(o) * depth, 128), depth)

    def square_iota(size):
        return [lax.broadcasted_iota(jnp.int32, (size, size), d) for d in (0, 1)]

    def pick(values, axis):
        low, high = (lax.slice_in_dim(values, i * per_group, (i + 1) * per_group, axis=axis) for i in range(2))
        return jnp.where(core == 0, low, high)

    def column(ref):
        i, j = square_iota(heads)
        mine = pick(jnp.sum(jnp.where(i == j, ref[...], 0.0), axis=1, keepdims=True), 0)
        return jnp.concatenate([mine, mine], axis=0)

    def my_positions(values):
        mine = values[:, 0:tok]
        for i in range(1, n_sp):
            mine = jnp.where(z == i, values[:, i * tok : (i + 1) * tok], mine)
        return mine

    for copy in small:
        copy.wait()
    other_seq = xe.at[pl.ds(pl.multiple_of((1 - core) * tok, 16), tok)]
    remote(x_hbm, other_seq, p_send.at[0], p_recv.at[0], partner).wait_recv()
    remote(stride_hbm, stride.at[1 - core], p_send.at[1], p_recv.at[1], partner).wait_recv()
    remote(damp_hbm.at[0, other_heads], damp.at[1 - core], p_send.at[2], p_recv.at[2], partner).wait_recv()

    raw = [pick(dot(wdt[...], xe[seq_rows(s), :], ((1,), (1,))), 0) for s in range(2)]
    raw = jnp.concatenate(raw, axis=0).astype(BF16).astype(F32)
    pre = raw + column(off)
    step_t = jnp.maximum(pre, 0.0) + jnp.log1p(jnp.exp(-jnp.abs(pre)))
    tempo = [jnp.broadcast_to(my_positions(stride[s]), (per_group, tok)) for s in range(2)]
    extra = [my_positions(damp[s]) for s in range(2)]
    keep = -column(rate) * step_t * jnp.concatenate(tempo, axis=0) + jnp.concatenate(extra, axis=0)
    row, col = square_iota(tok)
    lower = row >= col
    step = dot((row == col).astype(F32), step_t, ((1,), (1,)), HIGH)
    cum = dot(lower.astype(F32), keep, ((1,), (1,)), HIGH)
    cum_t = dot(keep, (row <= col).astype(F32), precision=HIGH)
    last = cum[tok - 1 : tok, :]
    to_end = jnp.exp(last - cum)
    reach = jnp.exp(cum)
    whole = jnp.exp(last)
    first_head = lax.broadcasted_iota(jnp.int32, (tok, 2 * P_SIZE), 1) < P_SIZE
    first_row = first_head[0:1, :]

    def spread(values, p, mask):
        return jnp.where(mask, values[:, 2 * p : 2 * p + 1], values[:, 2 * p + 1 : 2 * p + 2])

    def pair_cols(p):
        return pl.ds(p * 2 * P_SIZE, 2 * P_SIZE)

    pairs = per_group // 2
    main = pl.ds(0, 2 * tok)
    span = HALO + tok

    def near(w):
        own[w].wait()
        spot = bufs[w].at[partner_rows]
        remote(spot, spot, p_send.at[3 + w], p_recv.at[3 + w], partner).wait_recv()

    def tiles(width, tile, body):
        def run(j, carry):
            body(pl.ds(pl.multiple_of(j * tile, tile), tile))
            return carry

        lax.fori_loop(0, width // tile, run, 0)

    def near_z(cols):
        gz[:, cols] = dot(xe[main, chip_rows(0)], wz[chip_rows(0), cols])

    def put(buf, cols, values):
        for s in range(2):
            buf[pl.ds(s * span, HALO), cols] = values[2 * tok + s * HALO : 2 * tok + (s + 1) * HALO, :]
            buf[pl.ds(s * span + HALO, tok), cols] = values[s * tok : (s + 1) * tok, :]

    def conv(buf, s, cols, taps):
        first = s * span + HALO - CONV_W + 1
        total = taps[0:1, :] * buf[pl.ds(first, tok), cols]
        for k in range(1, CONV_W):
            total = total + taps[k : k + 1, :] * buf[pl.ds(first + k, tok), cols]
        return silu(total).astype(BF16)

    skip_vals = []

    def near_x(cols):
        px[:, cols] = dot(xe[:, chip_rows(0)], wx[chip_rows(0), cols])

    def maps_task():
        @pl.when(z == 0)
        def _():
            xe[pl.ds(2 * tok, 2 * HALO), :] = jnp.zeros((2 * HALO, xe.shape[1]), BF16)

        @pl.when(z > 0)
        def _():
            spot = xe.at[pl.ds(2 * tok, 2 * HALO)]
            remote(spot, spot, halo_send, halo_recv, partner).wait_recv()

        for copy in maps:
            copy.wait()
        put(pbc, pl.ds(0, 2 * N), dot(xe[...], wbc[...]).astype(BF16).astype(F32))
        for s in range(2):
            bm[seq_rows(s), :] = conv(pbc, s, pl.ds(0, N), tb[...])
            cm[seq_rows(s), :] = conv(pbc, s, pl.ds(N, N), tc[...])
        for s in range(2):
            cb[s] = dot(cm[seq_rows(s), :], bm[seq_rows(s), :], ((1,), (1,)))
        for copy in late:
            copy.wait()
        skip_vals.append(pick(skip[...], 1))

    def far_x(cols):
        acc = px[:, cols]
        for o in range(1, n_x):
            acc = acc + dot(xe[:, chip_rows(o)], wx[chip_rows(o), cols])
        put(pcx, cols, acc.astype(BF16).astype(F32))
        for s in range(2):
            xs[seq_rows(s), cols] = conv(pcx, s, cols, tx[:, cols])

    def far_z(cols):
        acc = gz[:, cols]
        for o in range(1, n_x):
            acc = acc + dot(xe[main, chip_rows(o)], wz[chip_rows(o), cols])
        gz[:, cols] = silu(acc.astype(BF16).astype(F32))

    def chain_copy(s, p):
        pc = pair_cols(p)
        return remote(
            snd.at[s, :, pc], car.at[s, :, pc], c_send, c_recv.at[s, p],
            {"sp": jnp.minimum(z + 1, n_sp - 1)},
        )

    def step_pairs(cols):
        return range(cols.start // (2 * P_SIZE), (cols.start + cols.size) // (2 * P_SIZE))

    def local_state(cols):
        for s in range(2):
            for p in step_pairs(cols):
                pc = pair_cols(p)
                v = s * pairs + p
                part = (xs[seq_rows(s), pc].astype(F32) * spread(step, v, first_head)).astype(BF16)
                scl[seq_rows(s), pc] = part
                sc[seq_rows(s), pc] = (part.astype(F32) * spread(to_end, v, first_head)).astype(BF16)
            st[s, :, cols] = dot(bm[seq_rows(s), :], sc[seq_rows(s), cols], ((0,), (0,)))

        @pl.when(z == 0)
        def _():
            for s in range(2):
                car[s, :, cols] = jnp.zeros((N, cols.size), BF16)
                for p in step_pairs(cols):
                    pc = pair_cols(p)
                    snd[s, :, pc] = st[s, :, pc].astype(BF16)
                    chain_copy(s, p).start()

    def chain(cols):
        for s in range(2):
            for p in step_pairs(cols):
                chain_copy(s, p).wait_recv()

                @pl.when(z < n_sp - 1)
                def _(s=s, p=p):
                    pc = pair_cols(p)
                    v = s * pairs + p
                    total = spread(whole, v, first_row) * car[s, :, pc].astype(F32) + st[s, :, pc]
                    snd[s, :, pc] = total.astype(BF16)
                    chain_copy(s, p).start()

    def chain_slot(slot, cols):
        @pl.when(jnp.minimum(z, 3) == slot)
        def _():
            chain(cols)

    def inner(s, cols):
        for p in step_pairs(cols):
            pc = pair_cols(p)
            parts = []
            for v in (s * per_group + 2 * p, s * per_group + 2 * p + 1):
                gap = jnp.where(lower, cum[:, v : v + 1] - cum_t[v : v + 1, :], -jnp.inf)
                parts.append(dot((cb[s] * jnp.exp(gap)).astype(BF16), scl[seq_rows(s), pc]))
            bypass = spread(skip_vals[0], p, first_row) * xs[seq_rows(s), pc].astype(F32)
            y[seq_rows(s), pc] = jnp.where(first_head, parts[0], parts[1]) + bypass

    def step_cols(s):
        return pl.ds(steps[s][1] * steps[s][2], steps[s][2])

    dp_pair = (dp, xi * 2 + 1 - core)

    def seq_rows_of(mine):
        return pl.ds(pl.multiple_of((core if mine else 1 - core) * tok, 16), tok)

    def finish(mine):
        seq = core if mine else 1 - core
        rows = seq_rows_of(mine)
        reached = dot(cm[rows, :], car[seq])
        reach_s = jnp.where(seq == 0, reach[:, 0:per_group], reach[:, per_group : 2 * per_group])
        square = jnp.zeros((tok, 1), F32)
        for p in range(pairs):
            pc = pair_cols(p)
            here = slice(p * 2 * P_SIZE, (p + 1) * 2 * P_SIZE)
            mixed = y[rows, pc] + spread(reach_s, p, first_head) * reached[:, here]
            gated = mixed.astype(BF16).astype(F32) * gz[rows, pc]
            square = square + jnp.sum(gated * gated, axis=1, keepdims=True)
            y[rows, pc] = gated
        inv = lax.rsqrt(square * (1.0 / gw) + EPSILON)
        normed = (y[rows, :] * inv * scale[...]).astype(BF16)
        if mine:
            nrm[:, own_cols] = normed
        else:
            nsn[...] = normed
            remote(nsn, nrm.at[:, own_cols], n_send, n_recv.at[0], partner).start()

    def half_k(d, cols, group_cols):
        first = pl.multiple_of(d * width + group_cols.start, 128)
        return dot(nrm[:, group_cols], wf[pl.ds(first, gw), cols])

    def out_a():
        own[2].wait()
        spot = wf.at[out_rows(dp_pair[1])]
        remote(spot, spot, p_send.at[5], p_recv.at[5], partner).wait_recv()
        for i, d in enumerate(dp_pair):
            for j in range(0, fw, tile):
                cols = pl.ds(j, tile)
                acc[i, :, cols] = half_k(d, cols, own_cols)

    def out_b():
        spot = nrm.at[:, other_cols]
        remote(nsn, spot, n_send, n_recv.at[0], partner).wait_recv()
        for i, d in enumerate(dp_pair):
            for j in range(0, fw, tile):
                cols = pl.ds(j, tile)
                whole_cols = pl.ds(pl.multiple_of(d * fw + j, 128), tile)
                out_ref[:, whole_cols] = (acc[i, :, cols] + half_k(d, cols, other_cols)).astype(BF16)

    def forward_copy(o, s):
        spot = wf.at[out_rows(owner_of(o) * 2 + core), step_cols(s)]
        return remote(spot, spot, f_send, f_recv.at[f_steps.index(s)], partner)

    def forward(s):
        rest(s)
        for o in range(1, n_x):
            forward_copy(o, s).start()

    def output(s):
        cols = step_cols(s)
        spot = wf.at[pl.ds(0, (n_x - 1) * width), cols]
        remote(spot, spot, f_send, f_recv.at[f_steps.index(s)], partner).wait_recv()
        for o in range(1, n_x):
            for d in (core, 1 - core):
                owner = owner_of(o) * 2 + d
                whole_cols = pl.ds(pl.multiple_of(owner * fw + cols.start, 128), cols.size)
                out_ref[:, whole_cols] = dot(nrm[...], wf[out_rows(owner), cols]).astype(BF16)

    f_steps = [s for s in range(len(steps)) if steps[s][0] == 2]
    tile = min(256, fw)

    def run(name):
        if name == "nearz":
            near(1)
            tiles(gw, 256, near_z)
        elif name == "pbc":
            maps_task()
        elif name == "nearx":
            near(0)
            tiles(gw, 256, near_x)
        elif name == "finishp":
            finish(False)
        elif name == "finisho":
            finish(True)
        elif name == "outa":
            out_a()
        elif name == "outb":
            out_b()
        else:
            task, s = name
            cols = step_cols(s)
            if task == "seeds":
                seeds(s)
            elif task in ("relay0", "relay1"):
                relay(s, int(task[-1]))
            elif task == "farx":
                rest(s)
                far_x(cols)
            elif task == "state":
                local_state(cols)
            elif task == "inner":
                for q in range(2):
                    inner(q, cols)
            elif task == "farz":
                rest(s)
                far_z(cols)
            elif task == "fwd":
                forward(s)
            else:
                output(s)

    for n, name in enumerate(order):
        for level in (1, 2, 3):
            for s, at in slots[level]:
                if at == n:
                    chain_slot(level, step_cols(s))
        run(name)

    def sent_wait(send, rows):
        if rows:
            spot = wx.at[pl.ds(0, rows)]
            remote(spot, spot, send, n_recv.at[0], partner).wait_send()

    for copy in sends:
        copy.wait_send()
    sent_wait(y_send, sent["y"])
    sent_wait(z_send, sent["z"])
    if sent["x"][0] == sent["x"][1]:
        sent_wait(x_send, sent["x"][0])
    else:
        for k in range(2):

            @pl.when(core == k)
            def _(k=k):
                sent_wait(x_send, sent["x"][k])

    remote(nsn, nsn, n_send, n_recv.at[0], partner).wait_send()
    spot = wf.at[pl.ds(0, (n_x - 1) * width)]
    remote(spot, spot, f_send, n_recv.at[0], partner).wait_send()

    @pl.when(z < n_sp - 1)
    def _():
        spot = xe.at[pl.ds(2 * tok, 2 * HALO)]
        remote(spot, spot, halo_send, halo_recv, partner).wait_send()
        remote(snd, snd, c_send, n_recv.at[0], partner).wait_send()


def shards(
    dims,
    mixer_source_array,
    source_projection,
    gating_projection,
    entry_mapping_projection,
    readout_mapping_projection,
    increment_projection,
    source_conv_taps,
    entry_mapping_taps,
    readout_mapping_taps,
    increment_offsets,
    channel_damping_rate,
    bypass_coefficients,
    stride_multiplier,
    added_log_damping,
    norm_scale_factor,
    final_projection,
):
    n_grp, n_sp, n_dp = dims
    n_x = n_dp // 2
    hidden = mixer_source_array[0]
    tok, model = hidden.shape
    width = source_projection.shape[1]
    gw = width // G
    heads = increment_projection.shape[1]
    fw = final_projection.shape[1]
    length = stride_multiplier.shape[1]
    out_width = fw * n_dp
    steps = plan(n_sp, n_x, gw, fw)[0]
    n_steps = len(steps)
    n_far = sum(1 for step in steps if step[0] == 2)
    span = HALO + tok
    dma = pltpu.SemaphoreType.DMA
    hbm = pl.BlockSpec(memory_space=pl.ANY)
    output = pl.pallas_call(
        functools.partial(kernel, dims),
        out_shape=pltpu.VMEM((tok, out_width), BF16),
        in_specs=[hbm] * 16,
        out_specs=pl.BlockSpec(memory_space=pltpu.VMEM),
        scratch_shapes=[
            pltpu.VMEM((2 * span, model), BF16),
            pltpu.VMEM((model, gw), BF16),
            pltpu.VMEM((model, gw), BF16),
            pltpu.VMEM((n_dp * width, fw), BF16),
            pltpu.VMEM((model, 2 * N), BF16),
            pltpu.VMEM((heads, model), BF16),
            pltpu.VMEM((CONV_W, gw), F32),
            pltpu.VMEM((CONV_W, N), F32),
            pltpu.VMEM((CONV_W, N), F32),
            pltpu.VMEM((1, heads), F32),
            pltpu.VMEM((1, heads), F32),
            pltpu.VMEM((1, heads), F32),
            pltpu.VMEM((2, 1, length), F32),
            pltpu.VMEM((2, heads // G, length), F32),
            pltpu.VMEM((1, gw), F32),
            pltpu.VMEM((2 * span, 2 * N), F32),
            pltpu.VMEM((2 * span, gw), F32),
            pltpu.VMEM((2 * span, gw), F32),
            pltpu.VMEM((2 * tok, gw), F32),
            pltpu.VMEM((2 * tok, N), BF16),
            pltpu.VMEM((2 * tok, N), BF16),
            pltpu.VMEM((2, tok, tok), F32),
            pltpu.VMEM((2 * tok, gw), BF16),
            pltpu.VMEM((2 * tok, gw), BF16),
            pltpu.VMEM((2 * tok, gw), BF16),
            pltpu.VMEM((2 * tok, gw), F32),
            pltpu.VMEM((2, N, gw), F32),
            pltpu.VMEM((2, N, gw), BF16),
            pltpu.VMEM((2, N, gw), BF16),
            pltpu.VMEM((tok, width), BF16),
            pltpu.VMEM((tok, gw), BF16),
            pltpu.VMEM((2, tok, fw), F32),
            dma((16,)),
            dma((6,)),
            dma((7,)),
            dma((7,)),
            dma((n_steps,)),
            dma((n_steps,)),
            dma((n_steps, 2)),
            dma((2, heads // G // 2)),
            dma((1,)),
            dma((n_far,)),
        ],
        compiler_params=pltpu.CompilerParams(
            collective_id=0, has_side_effects=True, vmem_limit_bytes=56 * 1024 * 1024
        ),
    )(
        hidden,
        source_projection,
        gating_projection,
        final_projection,
        entry_mapping_projection,
        readout_mapping_projection,
        increment_projection.T,
        source_conv_taps,
        entry_mapping_taps,
        readout_mapping_taps,
        increment_offsets[None],
        channel_damping_rate[None],
        bypass_coefficients[None],
        stride_multiplier,
        jnp.swapaxes(added_log_damping, 1, 2),
        norm_scale_factor[None],
    )
    return output[None]


def solution(mesh):
    n_grp, n_sp, n_dp = (mesh.shape[a] for a in ("grp", "sp", "dp"))
    return jax.shard_map(
        functools.partial(shards, (n_grp, n_sp, n_dp)),
        mesh=mesh,
        in_specs=(
            P(("grp", "dp"), "sp", None),
            P("dp", None),
            P("dp", None),
            P(),
            P(),
            P(),
            P(),
            P(),
            P(),
            P(),
            P(),
            P(),
            P(("grp", "dp"), None),
            P(("grp", "dp"), None, None),
            P(),
            P(None, "dp"),
        ),
        out_specs=P(("grp", "dp"), "sp", None),
        check_vma=False,
    )
```

```python
import functools

import jax
import jax.numpy as jnp
from jax import lax
from jax.experimental import pallas as pl
from jax.experimental.pallas import tpu as pltpu
from jax.sharding import PartitionSpec as P

P_SIZE = 64
N = 128
G = 2
CONV_W = 4
EPSILON = 1e-06
HIGH = lax.Precision.HIGHEST
MESH = pl.DeviceIdType.MESH
HALO = 16
CHUNKS = (128, 256, 128)
TYPES = (4, 2, 2, 4, 4, 3, 3, 4, 4, 2)
X_ORDER = (("S", 3), ("S", 1), ("S", 2), ("S", 0), ("E", 3), ("S", 5), ("S", 9), ("E", 0), ("S", 6), ("S", 4), ("S", 7), ("S", 8), ("E", 5), ("E", 4), ("E", 8), ("E", 6), ("E", 7))
ORDER = (
    ("seeds", 3),
    ("seeds", 1),
    ("seeds", 2),
    "pbc",
    ("relay0", 1),
    ("seeds", 0),
    "nearx",
    ("farx", 3),
    ("relay1", 1),
    ("state", 3),
    ("relay1", 2),
    ("relay0", 2),
    ("seeds", 5),
    ("seeds", 9),
    ("farx", 1),
    ("farx", 2),
    ("state", 2),
    ("inner", 3),
    ("farx", 0),
    ("relay0", 5),
    ("state", 1),
    ("state", 0),
    ("seeds", 6),
    ("seeds", 4),
    ("relay1", 9),
    "nearz",
    ("relay0", 9),
    ("inner", 0),
    ("seeds", 8),
    ("inner", 2),
    ("inner", 1),
    ("relay0", 6),
    ("farz", 5),
    ("seeds", 7),
    ("farz", 4),
    ("gate", 1),
    ("fwd", 8),
    ("fwd", 9),
    ("gate", 0),
    "finishp",
    "finisho",
    ("fwd", 6),
    ("fwd", 7),
    "outa",
    "outb",
    ("out", 1),
    ("out", 0),
)
SLOTS = (
    ((0, 24), (1, 33), (2, 30), (3, 27)),
    ((0, 29), (1, 26), (2, 23), (3, 13)),
    ((0, 33), (1, 30), (2, 28), (3, 19)),
    ((0, 38), (1, 37), (2, 35), (3, 24)),
)
F32 = jnp.float32
BF16 = jnp.bfloat16


def plan(n_sp, n_x, gw, fw):
    steps = []
    for w, wide in enumerate((gw, gw, fw)):
        cw = min(CHUNKS[w], wide)
        steps += [(w, j, cw) for j in range(wide // cw)]
    if (n_sp, n_x, len(steps)) == (4, 2, len(TYPES)):
        return steps, TYPES, X_ORDER, ORDER, SLOTS
    every = range(len(steps))
    x_order = [(kind, s) for s in every for kind in "SE"]
    order = ["nearz", "pbc", "nearx"]
    for s in every:
        order += [("seeds", s), ("relay0", s)]
        order += [[("farx", s), ("state", s), ("inner", s)], [("farz", s)], [("fwd", s)]][steps[s][0]]
    order += [("gate", j) for j in range(gw // 256)]
    order += ["finishp", "finisho", "outa", "outb"]
    order += [("out", j) for j in range(max(fw // 256, 1))]
    slots = [[(s, order.index(("gate", 0))) for s in every if steps[s][0] == 0]] * 4
    return steps, [3] * len(steps), x_order, order, slots


def dot(a, b, dims=((1,), (0,)), precision=None):
    return lax.dot_general(a, b, (dims, ((), ())), precision=precision, preferred_element_type=F32)


def silu(v):
    return v * (1.0 / (1.0 + jnp.exp(-v)))


def kernel(
    dims,
    x_hbm,
    wx_hbm,
    wz_hbm,
    wf_hbm,
    wb_hbm,
    wc_hbm,
    wdt_hbm,
    tx_hbm,
    tb_hbm,
    tc_hbm,
    off_hbm,
    rate_hbm,
    skip_hbm,
    stride_hbm,
    damp_hbm,
    scale_hbm,
    out_ref,
    xe,
    wx,
    wz,
    wf,
    wbc,
    wdt,
    tx,
    tb,
    tc,
    off,
    rate,
    skip,
    stride,
    damp,
    scale,
    pbc,
    px,
    pcx,
    gz,
    bm,
    cm,
    cb,
    xs,
    scl,
    sc,
    y,
    st,
    car,
    snd,
    nrm,
    nsn,
    acc,
    loc_sem,
    p_send,
    p_recv,
    link_send,
    seed_recv,
    rest_recv,
    relay_recv,
    c_recv,
    n_recv,
    f_recv,
):
    n_grp, n_sp, n_dp = dims
    n_x = n_dp // 2
    grp, z, dp = (lax.axis_index(a) for a in ("grp", "sp", "dp"))
    xi, core = dp // 2, dp % 2
    tok = out_ref.shape[0]
    heads = off.shape[1]
    per_group = heads // G
    gw = xs.shape[1]
    rows_dev = wx_hbm.shape[0]
    fw = wf_hbm.shape[1]
    width = wf_hbm.shape[0]
    halo_send, x_send, y_send, z_send, c_send, n_send, f_send = (link_send.at[i] for i in range(7))
    halo_recv = p_recv.at[6]
    own_cols = pl.ds(pl.multiple_of(core * gw, 128), gw)
    other_cols = pl.ds(pl.multiple_of((1 - core) * gw, 128), gw)
    partner = {"dp": xi * 2 + 1 - core}
    y_peer = {"grp": 1 - grp}
    zb = z % 2
    z_peer = {"sp": z + 1 - 2 * zb}
    bufs = (wx, wz, wf)
    srcs = (wx_hbm, wz_hbm, wf_hbm)
    own_q = grp * 2 + zb
    y_q = (1 - grp) * 2 + zb
    z_q = grp * 2 + 1 - zb
    far_q = (1 - grp) * 2 + 1 - zb

    barrier = pltpu.get_barrier_semaphore()

    def greet(peer):
        pl.semaphore_signal(barrier, inc=1, device_id=peer, device_id_type=MESH)

    greet(partner)
    greet(y_peer)
    for o in range(1, n_x):
        for d in range(2):
            greet({"dp": lax.rem(xi + o, n_x) * 2 + d})

    @pl.when(z > 0)
    def _():
        for d in range(2):
            greet({"sp": z - 1, "dp": xi * 2 + d})

    @pl.when(z < n_sp - 1)
    def _():
        for d in range(2):
            greet({"sp": z + 1, "dp": xi * 2 + d})

    def remote(src, dst, send, recv, peer):
        return pltpu.make_async_remote_copy(
            src_ref=src, dst_ref=dst, send_sem=send, recv_sem=recv,
            device_id=peer, device_id_type=MESH,
        )

    locals_ = []

    def local(src, dst):
        copy = pltpu.make_async_copy(src, dst, loc_sem.at[len(locals_)])
        copy.start()
        locals_.append(copy)
        return copy

    def out_rows(d):
        return pl.ds(pl.multiple_of(d * width, 128), width)

    def seq_rows(s):
        return pl.ds(s * tok, tok)

    dyn_rows = pl.ds(pl.multiple_of(core * tok, 16), tok)
    head_rows = pl.ds(pl.multiple_of(core * per_group, 8), per_group)
    other_heads = pl.ds(pl.multiple_of((1 - core) * per_group, 8), per_group)
    dev_rows = pl.ds(pl.multiple_of(dp * rows_dev, 16), rows_dev)
    partner_rows = pl.ds(pl.multiple_of((xi * 2 + 1 - core) * rows_dev, 16), rows_dev)
    group_n = pl.ds(pl.multiple_of(core * N, 128), N)

    small = [local(x_hbm, xe.at[dyn_rows])]
    small += [local(stride_hbm, stride.at[core]), local(damp_hbm.at[0, head_rows], damp.at[core])]
    small += [local(wdt_hbm, wdt), local(off_hbm, off), local(rate_hbm, rate)]
    maps = [local(wb_hbm.at[:, group_n], wbc.at[:, pl.ds(0, N)])]
    maps += [local(wc_hbm.at[:, group_n], wbc.at[:, pl.ds(N, N)])]
    maps += [local(tb_hbm.at[:, group_n], tb), local(tc_hbm.at[:, group_n], tc)]
    own = [local(srcs[w].at[:, own_cols], bufs[w].at[dev_rows]) for w in range(2)]
    own += [local(wf_hbm, wf.at[out_rows(dp)])]
    late = [local(tx_hbm.at[:, own_cols], tx), local(skip_hbm, skip), local(scale_hbm.at[:, own_cols], scale)]

    greeted = 2 + 2 * (n_x - 1) + 2 * jnp.minimum(z, 1) + 2 * jnp.minimum(n_sp - 1 - z, 1)
    pl.semaphore_wait(barrier, greeted)

    steps, types, x_order, order, slots = plan(n_sp, n_x, gw, fw)
    last_step = len(steps) - 1
    direct, relayed = [], []
    for kind in types:
        turn = sum(1 for d in direct if len(d) == 1) % 2
        direct.append({2: (), 3: (turn,), 4: (0, 1)}[kind])
        relayed.append(tuple(k for k in (0, 1) if k not in direct[-1]))

    relay_slots = [(s, k) for s in range(len(steps)) for k in relayed[s]]

    def relay_sem(s, k):
        return relay_recv.at[relay_slots.index((s, k))]

    def piece_rows(s):
        return width // 8 if steps[s][0] == 2 else rows_dev // 4

    def place(s, chip, q, k):
        w, j, cw = steps[s]
        size = piece_rows(s)
        row = (chip * 2 + core) * width + (q * 2 + k) * size if w == 2 else (chip * 2 + k) * rows_dev + q * size
        return bufs[w].at[pl.ds(pl.multiple_of(row, 16), size), pl.ds(j * cw, cw)]

    def origin(s, q, k, d):
        w, j, cw = steps[s]
        size = piece_rows(s)
        row, col = ((q * 2 + k) * size, j * cw) if w == 2 else (q * size, d * gw + j * cw)
        return srcs[w].at[pl.ds(pl.multiple_of(row, 16), size), pl.ds(pl.multiple_of(col, 128), cw)]

    def owner_of(o):
        return lax.rem(xi - o + n_x, n_x)

    sent = {"x": [0, 0], "y": 0, "z": 0}

    def x_start(s, o, q, k, d, recv):
        peer = {"dp": lax.rem(xi + o, n_x) * 2 + d}
        remote(origin(s, q, k, d), place(s, xi, q, k), x_send, recv.at[s], peer).start()

    def unit(s):
        return piece_rows(s) * steps[s][2] // gw

    def x_seeds(s):
        for o in range(1, n_x):
            if steps[s][0] == 2:
                for k in range(2):
                    x_start(s, o, own_q, k, core, seed_recv)
            else:
                for d in (core, 1 - core):
                    x_start(s, o, own_q, core, d, seed_recv)
            for k in range(2):
                sent["x"][k] += 2 * unit(s)

    def x_extras(s):
        for o in range(1, n_x):
            if steps[s][0] == 2:
                for k in direct[s]:
                    x_start(s, o, far_q, k, core, rest_recv)
                    sent["x"][0] += unit(s)
                    sent["x"][1] += unit(s)
            elif len(direct[s]) == 2:
                for d in (core, 1 - core):
                    x_start(s, o, far_q, core, d, rest_recv)
                sent["x"][0] += 2 * unit(s)
                sent["x"][1] += 2 * unit(s)
            else:
                for k in direct[s]:
                    sent["x"][k] += 2 * unit(s)

                    @pl.when(core == k)
                    def _(k=k, o=o):
                        for d in (core, 1 - core):
                            x_start(s, o, far_q, k, d, rest_recv)

    def y_start(s, o, q, k):
        spot = place(s, owner_of(o), q, k)
        remote(spot, spot, y_send, rest_recv.at[s], y_peer).start()
        sent["y"] += unit(s)

    def z_start(s, o, k):
        spot = place(s, owner_of(o), own_q, k)
        recv = relay_sem(s, k) if k in relayed[s] else rest_recv.at[s]
        remote(spot, spot, z_send, recv, z_peer).start()
        sent["z"] += unit(s)

    def pieces_wait(s, count, recv):
        w, j, cw = steps[s]
        spot = bufs[w].at[pl.ds(0, count * (n_x - 1) * piece_rows(s)), pl.ds(j * cw, cw)]
        remote(spot, spot, x_send, recv, partner).wait_recv()

    def halo_copies():
        up = jnp.minimum(z + 1, n_sp - 1)
        dst = xe.at[pl.ds(pl.multiple_of(2 * tok + core * HALO, 16), HALO)]
        src = x_hbm.at[pl.ds(tok - HALO, HALO)]
        return [remote(src, dst, halo_send, halo_recv, {"sp": up, "dp": xi * 2 + d}) for d in (core, 1 - core)]

    @pl.when(z < n_sp - 1)
    def _():
        for copy in halo_copies():
            copy.start()

    sends = []

    def start(copy):
        copy.start()
        sends.append(copy)

    for n, (kind, s) in enumerate(x_order):
        (x_seeds if kind == "S" else x_extras)(s)
        if n == 0:
            start(remote(x_hbm, xe.at[dyn_rows], p_send.at[0], p_recv.at[0], partner))
            start(remote(stride_hbm, stride.at[core], p_send.at[1], p_recv.at[1], partner))
            start(remote(damp_hbm.at[0, other_heads], damp.at[core], p_send.at[2], p_recv.at[2], partner))
            for w in range(2):
                start(remote(srcs[w].at[:, other_cols], bufs[w].at[dev_rows], p_send.at[3 + w], p_recv.at[3 + w], partner))
            start(remote(wf_hbm, wf.at[out_rows(dp)], p_send.at[5], p_recv.at[5], partner))

    def seeds(s):
        pieces_wait(s, 2, seed_recv.at[s])
        for o in range(1, n_x):
            for k in relayed[s] + direct[s]:
                z_start(s, o, k)
            for k in range(2):
                y_start(s, o, own_q, k)

    def relay(s, r):
        k = relayed[s][r]
        pieces_wait(s, 1, relay_sem(s, k))
        for o in range(1, n_x):
            y_start(s, o, z_q, k)

    def rest(s):
        pieces_wait(s, 6 - len(relayed[s]), rest_recv.at[s])

    depth = 2 * rows_dev

    def chip_rows(o):
        return pl.ds(pl.multiple_of(owner_of(o) * depth, 128), depth)

    def square_iota(size):
        return [lax.broadcasted_iota(jnp.int32, (size, size), d) for d in (0, 1)]

    def pick(values, axis):
        low, high = (lax.slice_in_dim(values, i * per_group, (i + 1) * per_group, axis=axis) for i in range(2))
        return jnp.where(core == 0, low, high)

    def column(ref):
        i, j = square_iota(heads)
        mine = pick(jnp.sum(jnp.where(i == j, ref[...], 0.0), axis=1, keepdims=True), 0)
        return jnp.concatenate([mine, mine], axis=0)

    def my_positions(values):
        mine = values[:, 0:tok]
        for i in range(1, n_sp):
            mine = jnp.where(z == i, values[:, i * tok : (i + 1) * tok], mine)
        return mine

    for copy in small:
        copy.wait()
    other_seq = xe.at[pl.ds(pl.multiple_of((1 - core) * tok, 16), tok)]
    remote(x_hbm, other_seq, p_send.at[0], p_recv.at[0], partner).wait_recv()
    remote(stride_hbm, stride.at[1 - core], p_send.at[1], p_recv.at[1], partner).wait_recv()
    remote(damp_hbm.at[0, other_heads], damp.at[1 - core], p_send.at[2], p_recv.at[2], partner).wait_recv()

    raw = [pick(dot(wdt[...], xe[seq_rows(s), :], ((1,), (1,))), 0) for s in range(2)]
    raw = jnp.concatenate(raw, axis=0).astype(BF16).astype(F32)
    pre = raw + column(off)
    step_t = jnp.maximum(pre, 0.0) + jnp.log1p(jnp.exp(-jnp.abs(pre)))
    tempo = [jnp.broadcast_to(my_positions(stride[s]), (per_group, tok)) for s in range(2)]
    extra = [my_positions(damp[s]) for s in range(2)]
    keep = -column(rate) * step_t * jnp.concatenate(tempo, axis=0) + jnp.concatenate(extra, axis=0)
    row, col = square_iota(tok)
    lower = row >= col
    step = dot((row == col).astype(F32), step_t, ((1,), (1,)), HIGH)
    cum = dot(lower.astype(F32), keep, ((1,), (1,)), HIGH)
    cum_t = dot(keep, (row <= col).astype(F32), precision=HIGH)
    last = cum[tok - 1 : tok, :]
    to_end = jnp.exp(last - cum)
    reach = jnp.exp(cum)
    whole = jnp.exp(last)
    first_head = lax.broadcasted_iota(jnp.int32, (tok, 2 * P_SIZE), 1) < P_SIZE
    first_row = first_head[0:1, :]

    def spread(values, p, mask):
        return jnp.where(mask, values[:, 2 * p : 2 * p + 1], values[:, 2 * p + 1 : 2 * p + 2])

    def pair_cols(p):
        return pl.ds(p * 2 * P_SIZE, 2 * P_SIZE)

    pairs = per_group // 2
    main = pl.ds(0, 2 * tok)
    span = HALO + tok

    def near(w):
        own[w].wait()
        spot = bufs[w].at[partner_rows]
        remote(spot, spot, p_send.at[3 + w], p_recv.at[3 + w], partner).wait_recv()

    def tiles(width, tile, body):
        def run(j, carry):
            body(pl.ds(pl.multiple_of(j * tile, tile), tile))
            return carry

        lax.fori_loop(0, width // tile, run, 0)

    def near_z(cols):
        gz[:, cols] = dot(xe[main, chip_rows(0)], wz[chip_rows(0), cols])

    def put(buf, cols, values):
        for s in range(2):
            buf[pl.ds(s * span, HALO), cols] = values[2 * tok + s * HALO : 2 * tok + (s + 1) * HALO, :]
            buf[pl.ds(s * span + HALO, tok), cols] = values[s * tok : (s + 1) * tok, :]

    def conv(buf, s, cols, taps):
        first = s * span + HALO - CONV_W + 1
        total = taps[0:1, :] * buf[pl.ds(first, tok), cols]
        for k in range(1, CONV_W):
            total = total + taps[k : k + 1, :] * buf[pl.ds(first + k, tok), cols]
        return silu(total).astype(BF16)

    skip_vals = []

    def near_x(cols):
        px[:, cols] = dot(xe[:, chip_rows(0)], wx[chip_rows(0), cols])

    def maps_task():
        @pl.when(z == 0)
        def _():
            xe[pl.ds(2 * tok, 2 * HALO), :] = jnp.zeros((2 * HALO, xe.shape[1]), BF16)

        @pl.when(z > 0)
        def _():
            spot = xe.at[pl.ds(2 * tok, 2 * HALO)]
            remote(spot, spot, halo_send, halo_recv, partner).wait_recv()

        for copy in maps:
            copy.wait()
        put(pbc, pl.ds(0, 2 * N), dot(xe[...], wbc[...]).astype(BF16).astype(F32))
        for s in range(2):
            bm[seq_rows(s), :] = conv(pbc, s, pl.ds(0, N), tb[...])
            cm[seq_rows(s), :] = conv(pbc, s, pl.ds(N, N), tc[...])
        for s in range(2):
            cb[s] = dot(cm[seq_rows(s), :], bm[seq_rows(s), :], ((1,), (1,)))
        for copy in late:
            copy.wait()
        skip_vals.append(pick(skip[...], 1))

    def far_x(cols):
        acc = px[:, cols]
        for o in range(1, n_x):
            acc = acc + dot(xe[:, chip_rows(o)], wx[chip_rows(o), cols])
        put(pcx, cols, acc.astype(BF16).astype(F32))
        for s in range(2):
            xs[seq_rows(s), cols] = conv(pcx, s, cols, tx[:, cols])

    def far_z(cols):
        acc = gz[:, cols]
        for o in range(1, n_x):
            acc = acc + dot(xe[main, chip_rows(o)], wz[chip_rows(o), cols])
        gz[:, cols] = silu(acc.astype(BF16).astype(F32))

    def chain_copy(s, p):
        pc = pair_cols(p)
        return remote(
            snd.at[s, :, pc], car.at[s, :, pc], c_send, c_recv.at[s, p],
            {"sp": jnp.minimum(z + 1, n_sp - 1)},
        )

    def step_pairs(cols):
        return range(cols.start // (2 * P_SIZE), (cols.start + cols.size) // (2 * P_SIZE))

    def local_state(cols):
        for s in range(2):
            for p in step_pairs(cols):
                pc = pair_cols(p)
                v = s * pairs + p
                part = (xs[seq_rows(s), pc].astype(F32) * spread(step, v, first_head)).astype(BF16)
                scl[seq_rows(s), pc] = part
                sc[seq_rows(s), pc] = (part.astype(F32) * spread(to_end, v, first_head)).astype(BF16)
            st[s, :, cols] = dot(bm[seq_rows(s), :], sc[seq_rows(s), cols], ((0,), (0,)))

        @pl.when(z == 0)
        def _():
            for s in range(2):
                car[s, :, cols] = jnp.zeros((N, cols.size), BF16)
                for p in step_pairs(cols):
                    pc = pair_cols(p)
                    snd[s, :, pc] = st[s, :, pc].astype(BF16)
                    chain_copy(s, p).start()

    def chain(cols):
        for s in range(2):
            for p in step_pairs(cols):
                chain_copy(s, p).wait_recv()

                @pl.when(z < n_sp - 1)
                def _(s=s, p=p):
                    pc = pair_cols(p)
                    v = s * pairs + p
                    total = spread(whole, v, first_row) * car[s, :, pc].astype(F32) + st[s, :, pc]
                    snd[s, :, pc] = total.astype(BF16)
                    chain_copy(s, p).start()

    def chain_slot(slot, cols):
        @pl.when(jnp.minimum(z, 3) == slot)
        def _():
            chain(cols)

    def inner(s, cols):
        for p in step_pairs(cols):
            pc = pair_cols(p)
            parts = []
            for v in (s * per_group + 2 * p, s * per_group + 2 * p + 1):
                gap = jnp.where(lower, cum[:, v : v + 1] - cum_t[v : v + 1, :], -jnp.inf)
                parts.append(dot((cb[s] * jnp.exp(gap)).astype(BF16), scl[seq_rows(s), pc]))
            bypass = spread(skip_vals[0], p, first_row) * xs[seq_rows(s), pc].astype(F32)
            y[seq_rows(s), pc] = jnp.where(first_head, parts[0], parts[1]) + bypass

    def step_cols(s):
        return pl.ds(steps[s][1] * steps[s][2], steps[s][2])

    dp_pair = (dp, xi * 2 + 1 - core)

    def seq_rows_of(mine):
        return pl.ds(pl.multiple_of((core if mine else 1 - core) * tok, 16), tok)

    def gate(j):
        cols = pl.ds(j * block, block)
        for s in range(2):
            reached = dot(cm[seq_rows(s), :], car[s, :, cols])
            for p in step_pairs(cols):
                pc = pair_cols(p)
                here = slice(p * 2 * P_SIZE - cols.start, (p + 1) * 2 * P_SIZE - cols.start)
                mixed = y[seq_rows(s), pc] + spread(reach, s * pairs + p, first_head) * reached[:, here]
                y[seq_rows(s), pc] = mixed.astype(BF16).astype(F32) * gz[seq_rows(s), pc]

    def finish(mine):
        gated = y[seq_rows_of(mine), :]
        square = jnp.sum(gated * gated, axis=1, keepdims=True)
        inv = lax.rsqrt(square * (1.0 / gw) + EPSILON)
        normed = (gated * inv * scale[...]).astype(BF16)
        if mine:
            nrm[:, own_cols] = normed
        else:
            nsn[...] = normed
            remote(nsn, nrm.at[:, own_cols], n_send, n_recv.at[0], partner).start()

    def half_k(d, cols, group_cols):
        first = pl.multiple_of(d * width + group_cols.start, 128)
        return dot(nrm[:, group_cols], wf[pl.ds(first, gw), cols])

    def out_a():
        own[2].wait()
        spot = wf.at[out_rows(dp_pair[1])]
        remote(spot, spot, p_send.at[5], p_recv.at[5], partner).wait_recv()
        for i, d in enumerate(dp_pair):
            for j in range(0, fw, tile):
                cols = pl.ds(j, tile)
                acc[i, :, cols] = half_k(d, cols, own_cols)

    def out_b():
        spot = nrm.at[:, other_cols]
        remote(nsn, spot, n_send, n_recv.at[0], partner).wait_recv()
        for i, d in enumerate(dp_pair):
            for j in range(0, fw, tile):
                cols = pl.ds(j, tile)
                whole_cols = pl.ds(pl.multiple_of(d * fw + j, 128), tile)
                out_ref[:, whole_cols] = (acc[i, :, cols] + half_k(d, cols, other_cols)).astype(BF16)

    def forward_copy(o, s):
        spot = wf.at[out_rows(owner_of(o) * 2 + core), step_cols(s)]
        return remote(spot, spot, f_send, f_recv.at[f_steps.index(s)], partner)

    def forward(s):
        rest(s)
        for o in range(1, n_x):
            forward_copy(o, s).start()

    def output(j):
        cols = pl.ds(j * tile, tile)
        for s in f_steps:
            if step_cols(s).start // tile == j:
                spot = wf.at[pl.ds(0, (n_x - 1) * width), step_cols(s)]
                remote(spot, spot, f_send, f_recv.at[f_steps.index(s)], partner).wait_recv()
        for o in range(1, n_x):
            for d in (core, 1 - core):
                owner = owner_of(o) * 2 + d
                whole_cols = pl.ds(pl.multiple_of(owner * fw + cols.start, 128), cols.size)
                out_ref[:, whole_cols] = dot(nrm[...], wf[out_rows(owner), cols]).astype(BF16)

    f_steps = [s for s in range(len(steps)) if steps[s][0] == 2]
    tile = min(256, fw)
    block = 256

    def run(name):
        if name == "nearz":
            near(1)
            tiles(gw, 256, near_z)
        elif name == "pbc":
            maps_task()
        elif name == "nearx":
            near(0)
            tiles(gw, 256, near_x)
        elif name == "finishp":
            finish(False)
        elif name == "finisho":
            finish(True)
        elif name == "outa":
            out_a()
        elif name == "outb":
            out_b()
        else:
            task, s = name
            if task == "seeds":
                seeds(s)
            elif task in ("relay0", "relay1"):
                relay(s, int(task[-1]))
            elif task == "farx":
                rest(s)
                far_x(step_cols(s))
            elif task == "state":
                local_state(step_cols(s))
            elif task == "inner":
                for q in range(2):
                    inner(q, step_cols(s))
            elif task == "farz":
                rest(s)
                far_z(step_cols(s))
            elif task == "gate":
                gate(s)
            elif task == "fwd":
                forward(s)
            else:
                output(s)

    for n, name in enumerate(order):
        for level in (1, 2, 3):
            for s, at in slots[level]:
                if at == n:
                    chain_slot(level, step_cols(s))
        run(name)

    def sent_wait(send, rows):
        if rows:
            spot = wx.at[pl.ds(0, rows)]
            remote(spot, spot, send, n_recv.at[0], partner).wait_send()

    for copy in sends:
        copy.wait_send()
    sent_wait(y_send, sent["y"])
    sent_wait(z_send, sent["z"])
    if sent["x"][0] == sent["x"][1]:
        sent_wait(x_send, sent["x"][0])
    else:
        for k in range(2):

            @pl.when(core == k)
            def _(k=k):
                sent_wait(x_send, sent["x"][k])

    remote(nsn, nsn, n_send, n_recv.at[0], partner).wait_send()
    spot = wf.at[pl.ds(0, (n_x - 1) * width)]
    remote(spot, spot, f_send, n_recv.at[0], partner).wait_send()

    @pl.when(z < n_sp - 1)
    def _():
        spot = xe.at[pl.ds(2 * tok, 2 * HALO)]
        remote(spot, spot, halo_send, halo_recv, partner).wait_send()
        remote(snd, snd, c_send, n_recv.at[0], partner).wait_send()


def shards(
    dims,
    mixer_source_array,
    source_projection,
    gating_projection,
    entry_mapping_projection,
    readout_mapping_projection,
    increment_projection,
    source_conv_taps,
    entry_mapping_taps,
    readout_mapping_taps,
    increment_offsets,
    channel_damping_rate,
    bypass_coefficients,
    stride_multiplier,
    added_log_damping,
    norm_scale_factor,
    final_projection,
):
    n_grp, n_sp, n_dp = dims
    n_x = n_dp // 2
    hidden = mixer_source_array[0]
    tok, model = hidden.shape
    width = source_projection.shape[1]
    gw = width // G
    heads = increment_projection.shape[1]
    fw = final_projection.shape[1]
    length = stride_multiplier.shape[1]
    out_width = fw * n_dp
    steps, types = plan(n_sp, n_x, gw, fw)[:2]
    n_relay = sum(4 - kind for kind in types)
    n_steps = len(steps)
    n_far = sum(1 for step in steps if step[0] == 2)
    span = HALO + tok
    dma = pltpu.SemaphoreType.DMA
    hbm = pl.BlockSpec(memory_space=pl.ANY)
    output = pl.pallas_call(
        functools.partial(kernel, dims),
        out_shape=pltpu.VMEM((tok, out_width), BF16),
        in_specs=[hbm] * 16,
        out_specs=pl.BlockSpec(memory_space=pltpu.VMEM),
        scratch_shapes=[
            pltpu.VMEM((2 * span, model), BF16),
            pltpu.VMEM((model, gw), BF16),
            pltpu.VMEM((model, gw), BF16),
            pltpu.VMEM((n_dp * width, fw), BF16),
            pltpu.VMEM((model, 2 * N), BF16),
            pltpu.VMEM((heads, model), BF16),
            pltpu.VMEM((CONV_W, gw), F32),
            pltpu.VMEM((CONV_W, N), F32),
            pltpu.VMEM((CONV_W, N), F32),
            pltpu.VMEM((1, heads), F32),
            pltpu.VMEM((1, heads), F32),
            pltpu.VMEM((1, heads), F32),
            pltpu.VMEM((2, 1, length), F32),
            pltpu.VMEM((2, heads // G, length), F32),
            pltpu.VMEM((1, gw), F32),
            pltpu.VMEM((2 * span, 2 * N), F32),
            pltpu.VMEM((2 * span, gw), F32),
            pltpu.VMEM((2 * span, gw), F32),
            pltpu.VMEM((2 * tok, gw), F32),
            pltpu.VMEM((2 * tok, N), BF16),
            pltpu.VMEM((2 * tok, N), BF16),
            pltpu.VMEM((2, tok, tok), F32),
            pltpu.VMEM((2 * tok, gw), BF16),
            pltpu.VMEM((2 * tok, gw), BF16),
            pltpu.VMEM((2 * tok, gw), BF16),
            pltpu.VMEM((2 * tok, gw), F32),
            pltpu.VMEM((2, N, gw), F32),
            pltpu.VMEM((2, N, gw), BF16),
            pltpu.VMEM((2, N, gw), BF16),
            pltpu.VMEM((tok, width), BF16),
            pltpu.VMEM((tok, gw), BF16),
            pltpu.VMEM((2, tok, fw), F32),
            dma((16,)),
            dma((6,)),
            dma((7,)),
            dma((7,)),
            dma((n_steps,)),
            dma((n_steps,)),
            dma((max(n_relay, 1),)),
            dma((2, heads // G // 2)),
            dma((1,)),
            dma((n_far,)),
        ],
        compiler_params=pltpu.CompilerParams(
            collective_id=0, has_side_effects=True, vmem_limit_bytes=56 * 1024 * 1024
        ),
    )(
        hidden,
        source_projection,
        gating_projection,
        final_projection,
        entry_mapping_projection,
        readout_mapping_projection,
        increment_projection.T,
        source_conv_taps,
        entry_mapping_taps,
        readout_mapping_taps,
        increment_offsets[None],
        channel_damping_rate[None],
        bypass_coefficients[None],
        stride_multiplier,
        jnp.swapaxes(added_log_damping, 1, 2),
        norm_scale_factor[None],
    )
    return output[None]


def solution(mesh):
    n_grp, n_sp, n_dp = (mesh.shape[a] for a in ("grp", "sp", "dp"))
    return jax.shard_map(
        functools.partial(shards, (n_grp, n_sp, n_dp)),
        mesh=mesh,
        in_specs=(
            P(("grp", "dp"), "sp", None),
            P("dp", None),
            P("dp", None),
            P(),
            P(),
            P(),
            P(),
            P(),
            P(),
            P(),
            P(),
            P(),
            P(("grp", "dp"), None),
            P(("grp", "dp"), None, None),
            P(),
            P(None, "dp"),
        ),
        out_specs=P(("grp", "dp"), "sp", None),
        check_vma=False,
    )
```

```python
import functools

import jax
import jax.numpy as jnp
from jax import lax
from jax.experimental import pallas as pl
from jax.experimental.pallas import tpu as pltpu
from jax.sharding import PartitionSpec as P

P_SIZE = 64
N = 128
G = 2
CONV_W = 4
EPSILON = 1e-06
HIGH = lax.Precision.HIGHEST
MESH = pl.DeviceIdType.MESH
HALO = 16
CHUNKS = (128, 256, 128)
TYPES = (4, 2, 4, 2, 4, 2, 4, 4, 4, 4)
ACROSS = (0, 0, 0, 0, 0, 0, 1, 0, 1, 0)
X_ORDER = (("S", 1), ("S", 3), ("S", 2), ("E", 2), ("S", 0), ("S", 5), ("E", 0), ("S", 8), ("S", 6), ("S", 4), ("S", 9), ("E", 8), ("E", 6), ("S", 7), ("E", 4), ("E", 9), ("E", 7))
ORDER = (
    ("seeds", 1),
    ("seeds", 3),
    ("seeds", 2),
    ("relay0", 1),
    "pbc",
    "nearx",
    ("relay0", 3),
    ("relay1", 3),
    ("seeds", 0),
    "nearz",
    ("relay1", 1),
    ("farx", 2),
    ("state", 2),
    ("seeds", 5),
    ("farx", 3),
    ("state", 3),
    ("farx", 0),
    ("state", 0),
    ("seeds", 8),
    ("farx", 1),
    ("state", 1),
    ("seeds", 6),
    ("relay1", 5),
    ("relay0", 5),
    ("seeds", 4),
    ("inner", 2),
    ("cross", 6),
    ("cross", 8),
    ("inner", 0),
    ("inner", 3),
    ("seeds", 9),
    ("seeds", 7),
    ("farz", 5),
    ("farz", 4),
    ("inner", 1),
    ("fwd", 6),
    ("gate", 1),
    ("fwd", 8),
    ("gate", 0),
    "finishp",
    ("fwd", 9),
    "finisho",
    ("fwd", 7),
    "outa",
    "outb",
    ("out", 1),
    ("out", 0),
)
SLOTS = (
    ((0, 22), (1, 28), (2, 26), (3, 20)),
    ((0, 26), (1, 30), (2, 16), (3, 22)),
    ((0, 29), (1, 31), (2, 22), (3, 28)),
    ((0, 36), (1, 38), (2, 32), (3, 32)),
)
F32 = jnp.float32
BF16 = jnp.bfloat16


def plan(n_sp, n_x, gw, fw):
    steps = []
    for w, wide in enumerate((gw, gw, fw)):
        cw = min(CHUNKS[w], wide)
        steps += [(w, j, cw) for j in range(wide // cw)]
    if (n_sp, n_x, len(steps)) == (4, 2, len(TYPES)):
        return steps, TYPES, ACROSS, X_ORDER, ORDER, SLOTS
    every = range(len(steps))
    x_order = [(kind, s) for s in every for kind in "SE"]
    order = ["nearz", "pbc", "nearx"]
    for s in every:
        order += [("seeds", s), ("relay0", s)]
        order += [[("farx", s), ("state", s), ("inner", s)], [("farz", s)], [("fwd", s)]][steps[s][0]]
    order += [("gate", j) for j in range(gw // 256)]
    order += ["finishp", "finisho", "outa", "outb"]
    order += [("out", j) for j in range(max(fw // 256, 1))]
    slots = [[(s, order.index(("gate", 0))) for s in every if steps[s][0] == 0]] * 4
    return steps, [3] * len(steps), [0] * len(steps), x_order, order, slots


def dot(a, b, dims=((1,), (0,)), precision=None):
    return lax.dot_general(a, b, (dims, ((), ())), precision=precision, preferred_element_type=F32)


def silu(v):
    return v * (1.0 / (1.0 + jnp.exp(-v)))


def kernel(
    dims,
    x_hbm,
    wx_hbm,
    wz_hbm,
    wf_hbm,
    wb_hbm,
    wc_hbm,
    wdt_hbm,
    tx_hbm,
    tb_hbm,
    tc_hbm,
    off_hbm,
    rate_hbm,
    skip_hbm,
    stride_hbm,
    damp_hbm,
    scale_hbm,
    out_ref,
    xe,
    wx,
    wz,
    wf,
    wbc,
    wdt,
    tx,
    tb,
    tc,
    off,
    rate,
    skip,
    stride,
    damp,
    scale,
    pbc,
    px,
    pcx,
    gz,
    bm,
    cm,
    cb,
    xs,
    scl,
    sc,
    y,
    st,
    car,
    snd,
    nrm,
    nsn,
    acc,
    loc_sem,
    p_send,
    p_recv,
    link_send,
    seed_recv,
    rest_recv,
    relay_recv,
    c_recv,
    n_recv,
    f_recv,
):
    n_grp, n_sp, n_dp = dims
    n_x = n_dp // 2
    grp, z, dp = (lax.axis_index(a) for a in ("grp", "sp", "dp"))
    xi, core = dp // 2, dp % 2
    tok = out_ref.shape[0]
    heads = off.shape[1]
    per_group = heads // G
    gw = xs.shape[1]
    rows_dev = wx_hbm.shape[0]
    fw = wf_hbm.shape[1]
    width = wf_hbm.shape[0]
    halo_send, x_send, y_send, z_send, c_send, n_send, f_send = (link_send.at[i] for i in range(7))
    halo_recv = p_recv.at[6]
    own_cols = pl.ds(pl.multiple_of(core * gw, 128), gw)
    other_cols = pl.ds(pl.multiple_of((1 - core) * gw, 128), gw)
    partner = {"dp": xi * 2 + 1 - core}
    y_peer = {"grp": 1 - grp}
    zb = z % 2
    z_peer = {"sp": z + 1 - 2 * zb}
    bufs = (wx, wz, wf)
    srcs = (wx_hbm, wz_hbm, wf_hbm)
    own_q = grp * 2 + zb
    y_q = (1 - grp) * 2 + zb
    z_q = grp * 2 + 1 - zb
    far_q = (1 - grp) * 2 + 1 - zb

    barrier = pltpu.get_barrier_semaphore()

    def greet(peer):
        pl.semaphore_signal(barrier, inc=1, device_id=peer, device_id_type=MESH)

    greet(partner)
    greet(y_peer)
    for o in range(1, n_x):
        for d in range(2):
            greet({"dp": lax.rem(xi + o, n_x) * 2 + d})

    @pl.when(z > 0)
    def _():
        for d in range(2):
            greet({"sp": z - 1, "dp": xi * 2 + d})

    @pl.when(z < n_sp - 1)
    def _():
        for d in range(2):
            greet({"sp": z + 1, "dp": xi * 2 + d})

    def remote(src, dst, send, recv, peer):
        return pltpu.make_async_remote_copy(
            src_ref=src, dst_ref=dst, send_sem=send, recv_sem=recv,
            device_id=peer, device_id_type=MESH,
        )

    locals_ = []

    def local(src, dst):
        copy = pltpu.make_async_copy(src, dst, loc_sem.at[len(locals_)])
        copy.start()
        locals_.append(copy)
        return copy

    def out_rows(d):
        return pl.ds(pl.multiple_of(d * width, 128), width)

    def seq_rows(s):
        return pl.ds(s * tok, tok)

    dyn_rows = pl.ds(pl.multiple_of(core * tok, 16), tok)
    head_rows = pl.ds(pl.multiple_of(core * per_group, 8), per_group)
    other_heads = pl.ds(pl.multiple_of((1 - core) * per_group, 8), per_group)
    dev_rows = pl.ds(pl.multiple_of(dp * rows_dev, 16), rows_dev)
    partner_rows = pl.ds(pl.multiple_of((xi * 2 + 1 - core) * rows_dev, 16), rows_dev)
    group_n = pl.ds(pl.multiple_of(core * N, 128), N)

    small = [local(x_hbm, xe.at[dyn_rows])]
    small += [local(stride_hbm, stride.at[core]), local(damp_hbm.at[0, head_rows], damp.at[core])]
    small += [local(wdt_hbm, wdt), local(off_hbm, off), local(rate_hbm, rate)]
    maps = [local(wb_hbm.at[:, group_n], wbc.at[:, pl.ds(0, N)])]
    maps += [local(wc_hbm.at[:, group_n], wbc.at[:, pl.ds(N, N)])]
    maps += [local(tb_hbm.at[:, group_n], tb), local(tc_hbm.at[:, group_n], tc)]
    own = [local(srcs[w].at[:, own_cols], bufs[w].at[dev_rows]) for w in range(2)]
    own += [local(wf_hbm, wf.at[out_rows(dp)])]
    late = [local(tx_hbm.at[:, own_cols], tx), local(skip_hbm, skip), local(scale_hbm.at[:, own_cols], scale)]

    greeted = 2 + 2 * (n_x - 1) + 2 * jnp.minimum(z, 1) + 2 * jnp.minimum(n_sp - 1 - z, 1)
    pl.semaphore_wait(barrier, greeted)

    steps, types, across, x_order, order, slots = plan(n_sp, n_x, gw, fw)
    last_step = len(steps) - 1
    direct, relayed = [], []
    for kind in types:
        turn = sum(1 for d in direct if len(d) == 1) % 2
        direct.append({2: (), 3: (turn,), 4: (0, 1)}[kind])
        relayed.append(tuple(k for k in (0, 1) if k not in direct[-1]))

    relay_slots = [(s, k) for s in range(len(steps)) for k in relayed[s]]
    relay_slots += [(s, "across") for s in range(len(steps)) if across[s]]

    def relay_sem(s, k):
        return relay_recv.at[relay_slots.index((s, k))]

    def piece_rows(s):
        return width // 8 if steps[s][0] == 2 else rows_dev // 4

    def place(s, chip, q, k):
        w, j, cw = steps[s]
        size = piece_rows(s)
        row = (chip * 2 + core) * width + (q * 2 + k) * size if w == 2 else (chip * 2 + k) * rows_dev + q * size
        return bufs[w].at[pl.ds(pl.multiple_of(row, 16), size), pl.ds(j * cw, cw)]

    def origin(s, q, k, d):
        w, j, cw = steps[s]
        size = piece_rows(s)
        row, col = ((q * 2 + k) * size, j * cw) if w == 2 else (q * size, d * gw + j * cw)
        return srcs[w].at[pl.ds(pl.multiple_of(row, 16), size), pl.ds(pl.multiple_of(col, 128), cw)]

    def owner_of(o):
        return lax.rem(xi - o + n_x, n_x)

    sent = {(c, b): 0 for c in range(2) for b in range(2)}
    sent.update(y=0, z=0, across=0)

    def x_start(s, o, q, k, d, recv):
        peer = {"dp": lax.rem(xi + o, n_x) * 2 + d}
        remote(origin(s, q, k, d), place(s, xi, q, k), x_send, recv.at[s], peer).start()

    def unit(s):
        return piece_rows(s) * steps[s][2] // gw

    def x_seeds(s):
        for o in range(1, n_x):
            if steps[s][0] == 2:
                for k in range(2):
                    x_start(s, o, own_q, k, core, seed_recv)
            else:
                for d in (core, 1 - core):
                    x_start(s, o, own_q, core, d, seed_recv)
            for key in ((0, 0), (0, 1), (1, 0), (1, 1)):
                sent[key] += 2 * unit(s)

    def x_extras(s):
        for o in range(1, n_x):
            for n, k in enumerate(direct[s]):
                odd_only = bool(across[s]) and n == 0
                near_only = steps[s][0] != 2
                sides = (1,) if odd_only else (0, 1)
                for c in (k,) if near_only else (0, 1):
                    for b in sides:
                        sent[c, b] += (2 if near_only else 1) * unit(s)

                def go(k=k, o=o):
                    for d in (core, 1 - core) if near_only else (core,):
                        x_start(s, o, far_q, k, d, rest_recv)

                if near_only and odd_only:
                    pl.when(jnp.logical_and(core == k, zb == 1))(go)
                elif near_only:
                    pl.when(core == k)(go)
                elif odd_only:
                    pl.when(zb == 1)(go)
                else:
                    go()

    def y_start(s, o, q, k, turned=False):
        spot = place(s, owner_of(o), q, k)
        recv = relay_sem(s, "across") if turned else rest_recv.at[s]
        remote(spot, spot, y_send, recv, y_peer).start()
        sent["y"] += unit(s)

    def z_start(s, o, k):
        spot = place(s, owner_of(o), own_q, k)
        recv = relay_sem(s, k) if k in relayed[s] else rest_recv.at[s]
        remote(spot, spot, z_send, recv, z_peer).start()
        sent["z"] += unit(s)

    def pieces_wait(s, count, recv):
        w, j, cw = steps[s]
        spot = bufs[w].at[pl.ds(0, count * (n_x - 1) * piece_rows(s)), pl.ds(j * cw, cw)]
        remote(spot, spot, x_send, recv, partner).wait_recv()

    def halo_copies():
        up = jnp.minimum(z + 1, n_sp - 1)
        dst = xe.at[pl.ds(pl.multiple_of(2 * tok + core * HALO, 16), HALO)]
        src = x_hbm.at[pl.ds(tok - HALO, HALO)]
        return [remote(src, dst, halo_send, halo_recv, {"sp": up, "dp": xi * 2 + d}) for d in (core, 1 - core)]

    @pl.when(z < n_sp - 1)
    def _():
        for copy in halo_copies():
            copy.start()

    sends = []

    def start(copy):
        copy.start()
        sends.append(copy)

    for n, (kind, s) in enumerate(x_order):
        (x_seeds if kind == "S" else x_extras)(s)
        if n == 0:
            start(remote(x_hbm, xe.at[dyn_rows], p_send.at[0], p_recv.at[0], partner))
            start(remote(stride_hbm, stride.at[core], p_send.at[1], p_recv.at[1], partner))
            start(remote(damp_hbm.at[0, other_heads], damp.at[core], p_send.at[2], p_recv.at[2], partner))
            for w in range(2):
                start(remote(srcs[w].at[:, other_cols], bufs[w].at[dev_rows], p_send.at[3 + w], p_recv.at[3 + w], partner))
            start(remote(wf_hbm, wf.at[out_rows(dp)], p_send.at[5], p_recv.at[5], partner))

    def seeds(s):
        pieces_wait(s, 2, seed_recv.at[s])
        for o in range(1, n_x):
            for k in relayed[s] + direct[s]:
                z_start(s, o, k)
            for k in direct[s] + relayed[s]:
                y_start(s, o, own_q, k, bool(across[s]) and k == direct[s][0])

    def cross(s):
        k = direct[s][0]
        pieces_wait(s, 1, relay_sem(s, "across"))
        sent["across"] += (n_x - 1) * unit(s)

        @pl.when(zb == 1)
        def _():
            for o in range(1, n_x):
                spot = place(s, owner_of(o), y_q, k)
                remote(spot, spot, z_send, rest_recv.at[s], z_peer).start()

    def relay(s, r):
        k = relayed[s][r]
        pieces_wait(s, 1, relay_sem(s, k))
        for o in range(1, n_x):
            y_start(s, o, z_q, k)

    def rest(s):
        pieces_wait(s, 6 - len(relayed[s]) - across[s], rest_recv.at[s])

    depth = 2 * rows_dev

    def chip_rows(o):
        return pl.ds(pl.multiple_of(owner_of(o) * depth, 128), depth)

    def square_iota(size):
        return [lax.broadcasted_iota(jnp.int32, (size, size), d) for d in (0, 1)]

    def pick(values, axis):
        low, high = (lax.slice_in_dim(values, i * per_group, (i + 1) * per_group, axis=axis) for i in range(2))
        return jnp.where(core == 0, low, high)

    def column(ref):
        i, j = square_iota(heads)
        mine = pick(jnp.sum(jnp.where(i == j, ref[...], 0.0), axis=1, keepdims=True), 0)
        return jnp.concatenate([mine, mine], axis=0)

    def my_positions(values):
        mine = values[:, 0:tok]
        for i in range(1, n_sp):
            mine = jnp.where(z == i, values[:, i * tok : (i + 1) * tok], mine)
        return mine

    for copy in small:
        copy.wait()
    other_seq = xe.at[pl.ds(pl.multiple_of((1 - core) * tok, 16), tok)]
    remote(x_hbm, other_seq, p_send.at[0], p_recv.at[0], partner).wait_recv()
    remote(stride_hbm, stride.at[1 - core], p_send.at[1], p_recv.at[1], partner).wait_recv()
    remote(damp_hbm.at[0, other_heads], damp.at[1 - core], p_send.at[2], p_recv.at[2], partner).wait_recv()

    raw = [pick(dot(wdt[...], xe[seq_rows(s), :], ((1,), (1,))), 0) for s in range(2)]
    raw = jnp.concatenate(raw, axis=0).astype(BF16).astype(F32)
    pre = raw + column(off)
    step_t = jnp.maximum(pre, 0.0) + jnp.log1p(jnp.exp(-jnp.abs(pre)))
    tempo = [jnp.broadcast_to(my_positions(stride[s]), (per_group, tok)) for s in range(2)]
    extra = [my_positions(damp[s]) for s in range(2)]
    keep = -column(rate) * step_t * jnp.concatenate(tempo, axis=0) + jnp.concatenate(extra, axis=0)
    row, col = square_iota(tok)
    lower = row >= col
    step = dot((row == col).astype(F32), step_t, ((1,), (1,)), HIGH)
    cum = dot(lower.astype(F32), keep, ((1,), (1,)), HIGH)
    cum_t = dot(keep, (row <= col).astype(F32), precision=HIGH)
    last = cum[tok - 1 : tok, :]
    to_end = jnp.exp(last - cum)
    reach = jnp.exp(cum)
    whole = jnp.exp(last)
    first_head = lax.broadcasted_iota(jnp.int32, (tok, 2 * P_SIZE), 1) < P_SIZE
    first_row = first_head[0:1, :]

    def spread(values, p, mask):
        return jnp.where(mask, values[:, 2 * p : 2 * p + 1], values[:, 2 * p + 1 : 2 * p + 2])

    def pair_cols(p):
        return pl.ds(p * 2 * P_SIZE, 2 * P_SIZE)

    pairs = per_group // 2
    main = pl.ds(0, 2 * tok)
    span = HALO + tok

    def near(w):
        own[w].wait()
        spot = bufs[w].at[partner_rows]
        remote(spot, spot, p_send.at[3 + w], p_recv.at[3 + w], partner).wait_recv()

    def tiles(width, tile, body):
        def run(j, carry):
            body(pl.ds(pl.multiple_of(j * tile, tile), tile))
            return carry

        lax.fori_loop(0, width // tile, run, 0)

    def near_z(cols):
        gz[:, cols] = dot(xe[main, chip_rows(0)], wz[chip_rows(0), cols])

    def put(buf, cols, values):
        for s in range(2):
            buf[pl.ds(s * span, HALO), cols] = values[2 * tok + s * HALO : 2 * tok + (s + 1) * HALO, :]
            buf[pl.ds(s * span + HALO, tok), cols] = values[s * tok : (s + 1) * tok, :]

    def conv(buf, s, cols, taps):
        first = s * span + HALO - CONV_W + 1
        total = taps[0:1, :] * buf[pl.ds(first, tok), cols]
        for k in range(1, CONV_W):
            total = total + taps[k : k + 1, :] * buf[pl.ds(first + k, tok), cols]
        return silu(total).astype(BF16)

    skip_vals = []

    def near_x(cols):
        px[:, cols] = dot(xe[:, chip_rows(0)], wx[chip_rows(0), cols])

    def maps_task():
        @pl.when(z == 0)
        def _():
            xe[pl.ds(2 * tok, 2 * HALO), :] = jnp.zeros((2 * HALO, xe.shape[1]), BF16)

        @pl.when(z > 0)
        def _():
            spot = xe.at[pl.ds(2 * tok, 2 * HALO)]
            remote(spot, spot, halo_send, halo_recv, partner).wait_recv()

        for copy in maps:
            copy.wait()
        put(pbc, pl.ds(0, 2 * N), dot(xe[...], wbc[...]).astype(BF16).astype(F32))
        for s in range(2):
            bm[seq_rows(s), :] = conv(pbc, s, pl.ds(0, N), tb[...])
            cm[seq_rows(s), :] = conv(pbc, s, pl.ds(N, N), tc[...])
        for s in range(2):
            cb[s] = dot(cm[seq_rows(s), :], bm[seq_rows(s), :], ((1,), (1,)))
        for copy in late:
            copy.wait()
        skip_vals.append(pick(skip[...], 1))

    def far_x(cols):
        acc = px[:, cols]
        for o in range(1, n_x):
            acc = acc + dot(xe[:, chip_rows(o)], wx[chip_rows(o), cols])
        put(pcx, cols, acc.astype(BF16).astype(F32))
        for s in range(2):
            xs[seq_rows(s), cols] = conv(pcx, s, cols, tx[:, cols])

    def far_z(cols):
        acc = gz[:, cols]
        for o in range(1, n_x):
            acc = acc + dot(xe[main, chip_rows(o)], wz[chip_rows(o), cols])
        gz[:, cols] = silu(acc.astype(BF16).astype(F32))

    def chain_copy(s, p):
        pc = pair_cols(p)
        return remote(
            snd.at[s, :, pc], car.at[s, :, pc], c_send, c_recv.at[s, p],
            {"sp": jnp.minimum(z + 1, n_sp - 1)},
        )

    def step_pairs(cols):
        return range(cols.start // (2 * P_SIZE), (cols.start + cols.size) // (2 * P_SIZE))

    def local_state(cols):
        for s in range(2):
            for p in step_pairs(cols):
                pc = pair_cols(p)
                v = s * pairs + p
                part = (xs[seq_rows(s), pc].astype(F32) * spread(step, v, first_head)).astype(BF16)
                scl[seq_rows(s), pc] = part
                sc[seq_rows(s), pc] = (part.astype(F32) * spread(to_end, v, first_head)).astype(BF16)
            st[s, :, cols] = dot(bm[seq_rows(s), :], sc[seq_rows(s), cols], ((0,), (0,)))

        @pl.when(z == 0)
        def _():
            for s in range(2):
                car[s, :, cols] = jnp.zeros((N, cols.size), BF16)
                for p in step_pairs(cols):
                    pc = pair_cols(p)
                    snd[s, :, pc] = st[s, :, pc].astype(BF16)
                    chain_copy(s, p).start()

    def chain(cols):
        for s in range(2):
            for p in step_pairs(cols):
                chain_copy(s, p).wait_recv()

                @pl.when(z < n_sp - 1)
                def _(s=s, p=p):
                    pc = pair_cols(p)
                    v = s * pairs + p
                    total = spread(whole, v, first_row) * car[s, :, pc].astype(F32) + st[s, :, pc]
                    snd[s, :, pc] = total.astype(BF16)
                    chain_copy(s, p).start()

    def chain_slot(slot, cols):
        @pl.when(jnp.minimum(z, 3) == slot)
        def _():
            chain(cols)

    def inner(s, cols):
        for p in step_pairs(cols):
            pc = pair_cols(p)
            parts = []
            for v in (s * per_group + 2 * p, s * per_group + 2 * p + 1):
                gap = jnp.where(lower, cum[:, v : v + 1] - cum_t[v : v + 1, :], -jnp.inf)
                parts.append(dot((cb[s] * jnp.exp(gap)).astype(BF16), scl[seq_rows(s), pc]))
            bypass = spread(skip_vals[0], p, first_row) * xs[seq_rows(s), pc].astype(F32)
            y[seq_rows(s), pc] = jnp.where(first_head, parts[0], parts[1]) + bypass

    def step_cols(s):
        return pl.ds(steps[s][1] * steps[s][2], steps[s][2])

    dp_pair = (dp, xi * 2 + 1 - core)

    def seq_rows_of(mine):
        return pl.ds(pl.multiple_of((core if mine else 1 - core) * tok, 16), tok)

    def gate(j):
        cols = pl.ds(j * block, block)
        for s in range(2):
            reached = dot(cm[seq_rows(s), :], car[s, :, cols])
            for p in step_pairs(cols):
                pc = pair_cols(p)
                here = slice(p * 2 * P_SIZE - cols.start, (p + 1) * 2 * P_SIZE - cols.start)
                mixed = y[seq_rows(s), pc] + spread(reach, s * pairs + p, first_head) * reached[:, here]
                y[seq_rows(s), pc] = mixed.astype(BF16).astype(F32) * gz[seq_rows(s), pc]

    def finish(mine):
        gated = y[seq_rows_of(mine), :]
        square = jnp.sum(gated * gated, axis=1, keepdims=True)
        inv = lax.rsqrt(square * (1.0 / gw) + EPSILON)
        normed = (gated * inv * scale[...]).astype(BF16)
        if mine:
            nrm[:, own_cols] = normed
        else:
            nsn[...] = normed
            remote(nsn, nrm.at[:, own_cols], n_send, n_recv.at[0], partner).start()

    def half_k(d, cols, group_cols):
        first = pl.multiple_of(d * width + group_cols.start, 128)
        return dot(nrm[:, group_cols], wf[pl.ds(first, gw), cols])

    def out_a():
        own[2].wait()
        spot = wf.at[out_rows(dp_pair[1])]
        remote(spot, spot, p_send.at[5], p_recv.at[5], partner).wait_recv()
        for i, d in enumerate(dp_pair):
            for j in range(0, fw, tile):
                cols = pl.ds(j, tile)
                acc[i, :, cols] = half_k(d, cols, own_cols)

    def out_b():
        spot = nrm.at[:, other_cols]
        remote(nsn, spot, n_send, n_recv.at[0], partner).wait_recv()
        for i, d in enumerate(dp_pair):
            for j in range(0, fw, tile):
                cols = pl.ds(j, tile)
                whole_cols = pl.ds(pl.multiple_of(d * fw + j, 128), tile)
                out_ref[:, whole_cols] = (acc[i, :, cols] + half_k(d, cols, other_cols)).astype(BF16)

    def forward_copy(o, s):
        spot = wf.at[out_rows(owner_of(o) * 2 + core), step_cols(s)]
        return remote(spot, spot, f_send, f_recv.at[f_steps.index(s)], partner)

    def forward(s):
        rest(s)
        for o in range(1, n_x):
            forward_copy(o, s).start()

    def output(j):
        cols = pl.ds(j * tile, tile)
        for s in f_steps:
            if step_cols(s).start // tile == j:
                spot = wf.at[pl.ds(0, (n_x - 1) * width), step_cols(s)]
                remote(spot, spot, f_send, f_recv.at[f_steps.index(s)], partner).wait_recv()
        for o in range(1, n_x):
            for d in (core, 1 - core):
                owner = owner_of(o) * 2 + d
                whole_cols = pl.ds(pl.multiple_of(owner * fw + cols.start, 128), cols.size)
                out_ref[:, whole_cols] = dot(nrm[...], wf[out_rows(owner), cols]).astype(BF16)

    f_steps = [s for s in range(len(steps)) if steps[s][0] == 2]
    tile = min(256, fw)
    block = 256

    def run(name):
        if name == "nearz":
            near(1)
            tiles(gw, 256, near_z)
        elif name == "pbc":
            maps_task()
        elif name == "nearx":
            near(0)
            tiles(gw, 256, near_x)
        elif name == "finishp":
            finish(False)
        elif name == "finisho":
            finish(True)
        elif name == "outa":
            out_a()
        elif name == "outb":
            out_b()
        else:
            task, s = name
            if task == "seeds":
                seeds(s)
            elif task == "cross":
                cross(s)
            elif task in ("relay0", "relay1"):
                relay(s, int(task[-1]))
            elif task == "farx":
                rest(s)
                far_x(step_cols(s))
            elif task == "state":
                local_state(step_cols(s))
            elif task == "inner":
                for q in range(2):
                    inner(q, step_cols(s))
            elif task == "farz":
                rest(s)
                far_z(step_cols(s))
            elif task == "gate":
                gate(s)
            elif task == "fwd":
                forward(s)
            else:
                output(s)

    for n, name in enumerate(order):
        for level in (1, 2, 3):
            for s, at in slots[level]:
                if at == n:
                    chain_slot(level, step_cols(s))
        run(name)

    def sent_wait(send, rows):
        if rows:
            spot = wx.at[pl.ds(0, rows)]
            remote(spot, spot, send, n_recv.at[0], partner).wait_send()

    for copy in sends:
        copy.wait_send()
    sent_wait(y_send, sent["y"])
    for b in range(2):

        @pl.when(zb == b)
        def _(b=b):
            sent_wait(z_send, sent["z"] + b * sent["across"])
            if sent[0, b] == sent[1, b]:
                sent_wait(x_send, sent[0, b])
            else:
                for c in range(2):

                    @pl.when(core == c)
                    def _(c=c):
                        sent_wait(x_send, sent[c, b])

    remote(nsn, nsn, n_send, n_recv.at[0], partner).wait_send()
    spot = wf.at[pl.ds(0, (n_x - 1) * width)]
    remote(spot, spot, f_send, n_recv.at[0], partner).wait_send()

    @pl.when(z < n_sp - 1)
    def _():
        spot = xe.at[pl.ds(2 * tok, 2 * HALO)]
        remote(spot, spot, halo_send, halo_recv, partner).wait_send()
        remote(snd, snd, c_send, n_recv.at[0], partner).wait_send()


def shards(
    dims,
    mixer_source_array,
    source_projection,
    gating_projection,
    entry_mapping_projection,
    readout_mapping_projection,
    increment_projection,
    source_conv_taps,
    entry_mapping_taps,
    readout_mapping_taps,
    increment_offsets,
    channel_damping_rate,
    bypass_coefficients,
    stride_multiplier,
    added_log_damping,
    norm_scale_factor,
    final_projection,
):
    n_grp, n_sp, n_dp = dims
    n_x = n_dp // 2
    hidden = mixer_source_array[0]
    tok, model = hidden.shape
    width = source_projection.shape[1]
    gw = width // G
    heads = increment_projection.shape[1]
    fw = final_projection.shape[1]
    length = stride_multiplier.shape[1]
    out_width = fw * n_dp
    steps, types, across = plan(n_sp, n_x, gw, fw)[:3]
    n_relay = sum(4 - kind for kind in types) + sum(across)
    n_steps = len(steps)
    n_far = sum(1 for step in steps if step[0] == 2)
    span = HALO + tok
    dma = pltpu.SemaphoreType.DMA
    hbm = pl.BlockSpec(memory_space=pl.ANY)
    output = pl.pallas_call(
        functools.partial(kernel, dims),
        out_shape=pltpu.VMEM((tok, out_width), BF16),
        in_specs=[hbm] * 16,
        out_specs=pl.BlockSpec(memory_space=pltpu.VMEM),
        scratch_shapes=[
            pltpu.VMEM((2 * span, model), BF16),
            pltpu.VMEM((model, gw), BF16),
            pltpu.VMEM((model, gw), BF16),
            pltpu.VMEM((n_dp * width, fw), BF16),
            pltpu.VMEM((model, 2 * N), BF16),
            pltpu.VMEM((heads, model), BF16),
            pltpu.VMEM((CONV_W, gw), F32),
            pltpu.VMEM((CONV_W, N), F32),
            pltpu.VMEM((CONV_W, N), F32),
            pltpu.VMEM((1, heads), F32),
            pltpu.VMEM((1, heads), F32),
            pltpu.VMEM((1, heads), F32),
            pltpu.VMEM((2, 1, length), F32),
            pltpu.VMEM((2, heads // G, length), F32),
            pltpu.VMEM((1, gw), F32),
            pltpu.VMEM((2 * span, 2 * N), F32),
            pltpu.VMEM((2 * span, gw), F32),
            pltpu.VMEM((2 * span, gw), F32),
            pltpu.VMEM((2 * tok, gw), F32),
            pltpu.VMEM((2 * tok, N), BF16),
            pltpu.VMEM((2 * tok, N), BF16),
            pltpu.VMEM((2, tok, tok), F32),
            pltpu.VMEM((2 * tok, gw), BF16),
            pltpu.VMEM((2 * tok, gw), BF16),
            pltpu.VMEM((2 * tok, gw), BF16),
            pltpu.VMEM((2 * tok, gw), F32),
            pltpu.VMEM((2, N, gw), F32),
            pltpu.VMEM((2, N, gw), BF16),
            pltpu.VMEM((2, N, gw), BF16),
            pltpu.VMEM((tok, width), BF16),
            pltpu.VMEM((tok, gw), BF16),
            pltpu.VMEM((2, tok, fw), F32),
            dma((16,)),
            dma((6,)),
            dma((7,)),
            dma((7,)),
            dma((n_steps,)),
            dma((n_steps,)),
            dma((max(n_relay, 1),)),
            dma((2, heads // G // 2)),
            dma((1,)),
            dma((n_far,)),
        ],
        compiler_params=pltpu.CompilerParams(
            collective_id=0, has_side_effects=True, vmem_limit_bytes=56 * 1024 * 1024
        ),
    )(
        hidden,
        source_projection,
        gating_projection,
        final_projection,
        entry_mapping_projection,
        readout_mapping_projection,
        increment_projection.T,
        source_conv_taps,
        entry_mapping_taps,
        readout_mapping_taps,
        increment_offsets[None],
        channel_damping_rate[None],
        bypass_coefficients[None],
        stride_multiplier,
        jnp.swapaxes(added_log_damping, 1, 2),
        norm_scale_factor[None],
    )
    return output[None]


def solution(mesh):
    n_grp, n_sp, n_dp = (mesh.shape[a] for a in ("grp", "sp", "dp"))
    return jax.shard_map(
        functools.partial(shards, (n_grp, n_sp, n_dp)),
        mesh=mesh,
        in_specs=(
            P(("grp", "dp"), "sp", None),
            P("dp", None),
            P("dp", None),
            P(),
            P(),
            P(),
            P(),
            P(),
            P(),
            P(),
            P(),
            P(),
            P(("grp", "dp"), None),
            P(("grp", "dp"), None, None),
            P(),
            P(None, "dp"),
        ),
        out_specs=P(("grp", "dp"), "sp", None),
        check_vma=False,
    )
```

```python
import functools

import jax
import jax.numpy as jnp
from jax import lax
from jax.experimental import pallas as pl
from jax.experimental.pallas import tpu as pltpu
from jax.sharding import PartitionSpec as P

P_SIZE = 64
N = 128
G = 2
CONV_W = 4
EPSILON = 1e-06
HIGH = lax.Precision.HIGHEST
MESH = pl.DeviceIdType.MESH
HALO = 16
CHUNKS = (128, 256, 128)
TYPES = (4, 2, 4, 2, 4, 2, 4, 4, 4, 4)
ACROSS = (0, 0, 0, 0, 0, 0, 1, 0, 1, 0)
X_ORDER = (("S", 1), ("S", 3), ("S", 2), ("E", 2), ("S", 0), ("S", 5), ("E", 0), ("S", 8), ("S", 6), ("S", 4), ("S", 9), ("E", 8), ("E", 6), ("S", 7), ("E", 4), ("E", 9), ("E", 7))
ORDER = (
    ("seeds", 1),
    ("seeds", 3),
    ("seeds", 2),
    ("relay0", 1),
    "pbc",
    "nearx",
    ("relay0", 3),
    ("relay1", 3),
    ("seeds", 0),
    "nearz",
    ("relay1", 1),
    ("farx", 2),
    ("state", 2),
    ("seeds", 5),
    ("farx", 3),
    ("state", 3),
    ("farx", 0),
    ("state", 0),
    ("seeds", 8),
    ("farx", 1),
    ("state", 1),
    ("seeds", 6),
    ("relay1", 5),
    ("relay0", 5),
    ("seeds", 4),
    ("inner", 2),
    ("cross", 6),
    ("cross", 8),
    ("inner", 0),
    ("inner", 3),
    ("seeds", 9),
    ("farz", 5),
    ("seeds", 7),
    ("farz", 4),
    ("inner", 1),
    ("fwd", 6),
    ("gate", 1),
    ("fwd", 8),
    ("gate", 0),
    "finishp",
    ("fwd", 9),
    "finisho",
    ("fwd", 7),
    "outa",
    "outb",
    ("out", 1),
    ("out", 0),
)
SLOTS = (
    ((0, 22), (1, 28), (2, 26), (3, 20)),
    ((0, 26), (1, 30), (2, 16), (3, 22)),
    ((0, 29), (1, 31), (2, 22), (3, 28)),
    ((0, 36), (1, 38), (2, 32), (3, 32)),
)
F32 = jnp.float32
BF16 = jnp.bfloat16


def plan(n_sp, n_x, gw, fw):
    steps = []
    for w, wide in enumerate((gw, gw, fw)):
        cw = min(CHUNKS[w], wide)
        steps += [(w, j, cw) for j in range(wide // cw)]
    if (n_sp, n_x, len(steps)) == (4, 2, len(TYPES)):
        return steps, TYPES, ACROSS, X_ORDER, ORDER, SLOTS
    every = range(len(steps))
    x_order = [(kind, s) for s in every for kind in "SE"]
    order = ["nearz", "pbc", "nearx"]
    for s in every:
        order += [("seeds", s), ("relay0", s)]
        order += [[("farx", s), ("state", s), ("inner", s)], [("farz", s)], [("fwd", s)]][steps[s][0]]
    order += [("gate", j) for j in range(gw // 256)]
    order += ["finishp", "finisho", "outa", "outb"]
    order += [("out", j) for j in range(max(fw // 256, 1))]
    slots = [[(s, order.index(("gate", 0))) for s in every if steps[s][0] == 0]] * 4
    return steps, [3] * len(steps), [0] * len(steps), x_order, order, slots


def dot(a, b, dims=((1,), (0,)), precision=None):
    return lax.dot_general(a, b, (dims, ((), ())), precision=precision, preferred_element_type=F32)


def silu(v):
    return v * (1.0 / (1.0 + jnp.exp(-v)))


def kernel(
    dims,
    x_hbm,
    wx_hbm,
    wz_hbm,
    wf_hbm,
    wb_hbm,
    wc_hbm,
    wdt_hbm,
    tx_hbm,
    tb_hbm,
    tc_hbm,
    off_hbm,
    rate_hbm,
    skip_hbm,
    stride_hbm,
    damp_hbm,
    scale_hbm,
    out_ref,
    xe,
    wx,
    wz,
    wf,
    wbc,
    wdt,
    tx,
    tb,
    tc,
    off,
    rate,
    skip,
    stride,
    damp,
    scale,
    pbc,
    px,
    pcx,
    gz,
    bm,
    cm,
    cb,
    xs,
    scl,
    sc,
    y,
    st,
    car,
    snd,
    nrm,
    nsn,
    acc,
    loc_sem,
    p_send,
    p_recv,
    link_send,
    seed_recv,
    rest_recv,
    relay_recv,
    c_recv,
    n_recv,
    f_recv,
):
    n_grp, n_sp, n_dp = dims
    n_x = n_dp // 2
    grp, z, dp = (lax.axis_index(a) for a in ("grp", "sp", "dp"))
    xi, core = dp // 2, dp % 2
    tok = out_ref.shape[0]
    heads = off.shape[1]
    per_group = heads // G
    gw = xs.shape[1]
    rows_dev = wx_hbm.shape[0]
    fw = wf_hbm.shape[1]
    width = wf_hbm.shape[0]
    halo_send, x_send, y_send, z_send, c_send, n_send, f_send = (link_send.at[i] for i in range(7))
    halo_recv = p_recv.at[6]
    own_cols = pl.ds(pl.multiple_of(core * gw, 128), gw)
    other_cols = pl.ds(pl.multiple_of((1 - core) * gw, 128), gw)
    partner = {"dp": xi * 2 + 1 - core}
    y_peer = {"grp": 1 - grp}
    zb = z % 2
    z_peer = {"sp": z + 1 - 2 * zb}
    bufs = (wx, wz, wf)
    srcs = (wx_hbm, wz_hbm, wf_hbm)
    own_q = grp * 2 + zb
    y_q = (1 - grp) * 2 + zb
    z_q = grp * 2 + 1 - zb
    far_q = (1 - grp) * 2 + 1 - zb

    barrier = pltpu.get_barrier_semaphore()

    def greet(peer):
        pl.semaphore_signal(barrier, inc=1, device_id=peer, device_id_type=MESH)

    greet(partner)
    greet(y_peer)
    for o in range(1, n_x):
        for d in range(2):
            greet({"dp": lax.rem(xi + o, n_x) * 2 + d})

    @pl.when(z > 0)
    def _():
        for d in range(2):
            greet({"sp": z - 1, "dp": xi * 2 + d})

    @pl.when(z < n_sp - 1)
    def _():
        for d in range(2):
            greet({"sp": z + 1, "dp": xi * 2 + d})

    def remote(src, dst, send, recv, peer):
        return pltpu.make_async_remote_copy(
            src_ref=src, dst_ref=dst, send_sem=send, recv_sem=recv,
            device_id=peer, device_id_type=MESH,
        )

    locals_ = []

    def local(src, dst):
        copy = pltpu.make_async_copy(src, dst, loc_sem.at[len(locals_)])
        copy.start()
        locals_.append(copy)
        return copy

    def out_rows(d):
        return pl.ds(pl.multiple_of(d * width, 128), width)

    def seq_rows(s):
        return pl.ds(s * tok, tok)

    dyn_rows = pl.ds(pl.multiple_of(core * tok, 16), tok)
    head_rows = pl.ds(pl.multiple_of(core * per_group, 8), per_group)
    other_heads = pl.ds(pl.multiple_of((1 - core) * per_group, 8), per_group)
    dev_rows = pl.ds(pl.multiple_of(dp * rows_dev, 16), rows_dev)
    partner_rows = pl.ds(pl.multiple_of((xi * 2 + 1 - core) * rows_dev, 16), rows_dev)
    group_n = pl.ds(pl.multiple_of(core * N, 128), N)

    small = [local(x_hbm, xe.at[dyn_rows])]
    small += [local(stride_hbm, stride.at[core]), local(damp_hbm.at[0, head_rows], damp.at[core])]
    small += [local(wdt_hbm, wdt), local(off_hbm, off), local(rate_hbm, rate)]
    maps = [local(wb_hbm.at[:, group_n], wbc.at[:, pl.ds(0, N)])]
    maps += [local(wc_hbm.at[:, group_n], wbc.at[:, pl.ds(N, N)])]
    maps += [local(tb_hbm.at[:, group_n], tb), local(tc_hbm.at[:, group_n], tc)]
    own = [local(srcs[w].at[:, own_cols], bufs[w].at[dev_rows]) for w in range(2)]
    own += [local(wf_hbm, wf.at[out_rows(dp)])]
    late = [local(tx_hbm.at[:, own_cols], tx), local(skip_hbm, skip), local(scale_hbm.at[:, own_cols], scale)]

    greeted = 2 + 2 * (n_x - 1) + 2 * jnp.minimum(z, 1) + 2 * jnp.minimum(n_sp - 1 - z, 1)
    pl.semaphore_wait(barrier, greeted)

    steps, types, across, x_order, order, slots = plan(n_sp, n_x, gw, fw)
    last_step = len(steps) - 1
    direct, relayed = [], []
    for kind in types:
        turn = sum(1 for d in direct if len(d) == 1) % 2
        direct.append({2: (), 3: (turn,), 4: (0, 1)}[kind])
        relayed.append(tuple(k for k in (0, 1) if k not in direct[-1]))

    relay_slots = [(s, k) for s in range(len(steps)) for k in relayed[s]]
    relay_slots += [(s, "across") for s in range(len(steps)) if across[s]]

    def relay_sem(s, k):
        return relay_recv.at[relay_slots.index((s, k))]

    def piece_rows(s):
        return width // 8 if steps[s][0] == 2 else rows_dev // 4

    def place(s, chip, q, k):
        w, j, cw = steps[s]
        size = piece_rows(s)
        row = (chip * 2 + core) * width + (q * 2 + k) * size if w == 2 else (chip * 2 + k) * rows_dev + q * size
        return bufs[w].at[pl.ds(pl.multiple_of(row, 16), size), pl.ds(j * cw, cw)]

    def origin(s, q, k, d):
        w, j, cw = steps[s]
        size = piece_rows(s)
        row, col = ((q * 2 + k) * size, j * cw) if w == 2 else (q * size, d * gw + j * cw)
        return srcs[w].at[pl.ds(pl.multiple_of(row, 16), size), pl.ds(pl.multiple_of(col, 128), cw)]

    def owner_of(o):
        return lax.rem(xi - o + n_x, n_x)

    sent = {(c, b): 0 for c in range(2) for b in range(2)}
    sent.update(y=0, z=0, across=0)

    def x_start(s, o, q, k, d, recv):
        peer = {"dp": lax.rem(xi + o, n_x) * 2 + d}
        remote(origin(s, q, k, d), place(s, xi, q, k), x_send, recv.at[s], peer).start()

    def unit(s):
        return piece_rows(s) * steps[s][2] // gw

    def x_seeds(s):
        for o in range(1, n_x):
            if steps[s][0] == 2:
                for k in range(2):
                    x_start(s, o, own_q, k, core, seed_recv)
            else:
                for d in (core, 1 - core):
                    x_start(s, o, own_q, core, d, seed_recv)
            for key in ((0, 0), (0, 1), (1, 0), (1, 1)):
                sent[key] += 2 * unit(s)

    def x_extras(s):
        for o in range(1, n_x):
            for n, k in enumerate(direct[s]):
                odd_only = bool(across[s]) and n == 0
                near_only = steps[s][0] != 2
                sides = (1,) if odd_only else (0, 1)
                for c in (k,) if near_only else (0, 1):
                    for b in sides:
                        sent[c, b] += (2 if near_only else 1) * unit(s)

                def go(k=k, o=o):
                    for d in (core, 1 - core) if near_only else (core,):
                        x_start(s, o, far_q, k, d, rest_recv)

                if near_only and odd_only:
                    pl.when(jnp.logical_and(core == k, zb == 1))(go)
                elif near_only:
                    pl.when(core == k)(go)
                elif odd_only:
                    pl.when(zb == 1)(go)
                else:
                    go()

    def y_start(s, o, q, k, turned=False):
        spot = place(s, owner_of(o), q, k)
        recv = relay_sem(s, "across") if turned else rest_recv.at[s]
        remote(spot, spot, y_send, recv, y_peer).start()
        sent["y"] += unit(s)

    def z_start(s, o, k):
        spot = place(s, owner_of(o), own_q, k)
        recv = relay_sem(s, k) if k in relayed[s] else rest_recv.at[s]
        remote(spot, spot, z_send, recv, z_peer).start()
        sent["z"] += unit(s)

    def pieces_wait(s, count, recv):
        w, j, cw = steps[s]
        spot = bufs[w].at[pl.ds(0, count * (n_x - 1) * piece_rows(s)), pl.ds(j * cw, cw)]
        remote(spot, spot, x_send, recv, partner).wait_recv()

    def halo_copies():
        up = jnp.minimum(z + 1, n_sp - 1)
        dst = xe.at[pl.ds(pl.multiple_of(2 * tok + core * HALO, 16), HALO)]
        src = x_hbm.at[pl.ds(tok - HALO, HALO)]
        return [remote(src, dst, halo_send, halo_recv, {"sp": up, "dp": xi * 2 + d}) for d in (core, 1 - core)]

    @pl.when(z < n_sp - 1)
    def _():
        for copy in halo_copies():
            copy.start()

    sends = []

    def start(copy):
        copy.start()
        sends.append(copy)

    for n, (kind, s) in enumerate(x_order):
        (x_seeds if kind == "S" else x_extras)(s)
        if n == 0:
            start(remote(x_hbm, xe.at[dyn_rows], p_send.at[0], p_recv.at[0], partner))
            start(remote(stride_hbm, stride.at[core], p_send.at[1], p_recv.at[1], partner))
            start(remote(damp_hbm.at[0, other_heads], damp.at[core], p_send.at[2], p_recv.at[2], partner))
            for w in range(2):
                remote(srcs[w].at[:, other_cols], bufs[w].at[dev_rows], p_send.at[3], p_recv.at[3 + w], partner).start()
            remote(wf_hbm, wf.at[out_rows(dp)], p_send.at[3], p_recv.at[5], partner).start()

    def seeds(s):
        pieces_wait(s, 2, seed_recv.at[s])
        for o in range(1, n_x):
            for k in relayed[s] + direct[s]:
                z_start(s, o, k)
            for k in direct[s] + relayed[s]:
                y_start(s, o, own_q, k, bool(across[s]) and k == direct[s][0])

    def cross(s):
        k = direct[s][0]
        pieces_wait(s, 1, relay_sem(s, "across"))
        sent["across"] += (n_x - 1) * unit(s)

        @pl.when(zb == 1)
        def _():
            for o in range(1, n_x):
                spot = place(s, owner_of(o), y_q, k)
                remote(spot, spot, z_send, rest_recv.at[s], z_peer).start()

    def relay(s, r):
        k = relayed[s][r]
        pieces_wait(s, 1, relay_sem(s, k))
        for o in range(1, n_x):
            y_start(s, o, z_q, k)

    def rest(s):
        pieces_wait(s, 6 - len(relayed[s]) - across[s], rest_recv.at[s])

    depth = 2 * rows_dev

    def chip_rows(o):
        return pl.ds(pl.multiple_of(owner_of(o) * depth, 128), depth)

    def square_iota(size):
        return [lax.broadcasted_iota(jnp.int32, (size, size), d) for d in (0, 1)]

    def pick(values, axis):
        low, high = (lax.slice_in_dim(values, i * per_group, (i + 1) * per_group, axis=axis) for i in range(2))
        return jnp.where(core == 0, low, high)

    def column(ref):
        i, j = square_iota(heads)
        mine = pick(jnp.sum(jnp.where(i == j, ref[...], 0.0), axis=1, keepdims=True), 0)
        return jnp.concatenate([mine, mine], axis=0)

    def my_positions(values):
        mine = values[:, 0:tok]
        for i in range(1, n_sp):
            mine = jnp.where(z == i, values[:, i * tok : (i + 1) * tok], mine)
        return mine

    for copy in small:
        copy.wait()
    other_seq = xe.at[pl.ds(pl.multiple_of((1 - core) * tok, 16), tok)]
    remote(x_hbm, other_seq, p_send.at[0], p_recv.at[0], partner).wait_recv()
    remote(stride_hbm, stride.at[1 - core], p_send.at[1], p_recv.at[1], partner).wait_recv()
    remote(damp_hbm.at[0, other_heads], damp.at[1 - core], p_send.at[2], p_recv.at[2], partner).wait_recv()

    raw = [pick(dot(wdt[...], xe[seq_rows(s), :], ((1,), (1,))), 0) for s in range(2)]
    raw = jnp.concatenate(raw, axis=0).astype(BF16).astype(F32)
    pre = raw + column(off)
    step_t = jnp.maximum(pre, 0.0) + jnp.log1p(jnp.exp(-jnp.abs(pre)))
    tempo = [jnp.broadcast_to(my_positions(stride[s]), (per_group, tok)) for s in range(2)]
    extra = [my_positions(damp[s]) for s in range(2)]
    keep = -column(rate) * step_t * jnp.concatenate(tempo, axis=0) + jnp.concatenate(extra, axis=0)
    row, col = square_iota(tok)
    lower = row >= col
    step = dot((row == col).astype(F32), step_t, ((1,), (1,)), HIGH)
    cum = dot(lower.astype(F32), keep, ((1,), (1,)), HIGH)
    cum_t = dot(keep, (row <= col).astype(F32), precision=HIGH)
    last = cum[tok - 1 : tok, :]
    to_end = jnp.exp(last - cum)
    reach = jnp.exp(cum)
    whole = jnp.exp(last)
    first_head = lax.broadcasted_iota(jnp.int32, (tok, 2 * P_SIZE), 1) < P_SIZE
    first_row = first_head[0:1, :]

    def spread(values, p, mask):
        return jnp.where(mask, values[:, 2 * p : 2 * p + 1], values[:, 2 * p + 1 : 2 * p + 2])

    def pair_cols(p):
        return pl.ds(p * 2 * P_SIZE, 2 * P_SIZE)

    pairs = per_group // 2
    main = pl.ds(0, 2 * tok)
    span = HALO + tok

    def near(w):
        own[w].wait()
        spot = bufs[w].at[partner_rows]
        remote(spot, spot, p_send.at[3], p_recv.at[3 + w], partner).wait_recv()

    def tiles(width, tile, body):
        def run(j, carry):
            body(pl.ds(pl.multiple_of(j * tile, tile), tile))
            return carry

        lax.fori_loop(0, width // tile, run, 0)

    def near_z(cols):
        gz[:, cols] = dot(xe[main, chip_rows(0)], wz[chip_rows(0), cols])

    def put(buf, cols, values):
        for s in range(2):
            buf[pl.ds(s * span, HALO), cols] = values[2 * tok + s * HALO : 2 * tok + (s + 1) * HALO, :]
            buf[pl.ds(s * span + HALO, tok), cols] = values[s * tok : (s + 1) * tok, :]

    def conv(buf, s, cols, taps):
        first = s * span + HALO - CONV_W + 1
        total = taps[0:1, :] * buf[pl.ds(first, tok), cols]
        for k in range(1, CONV_W):
            total = total + taps[k : k + 1, :] * buf[pl.ds(first + k, tok), cols]
        return silu(total).astype(BF16)

    skip_vals = []

    def near_x(cols):
        px[:, cols] = dot(xe[:, chip_rows(0)], wx[chip_rows(0), cols])

    def maps_task():
        @pl.when(z == 0)
        def _():
            xe[pl.ds(2 * tok, 2 * HALO), :] = jnp.zeros((2 * HALO, xe.shape[1]), BF16)

        @pl.when(z > 0)
        def _():
            spot = xe.at[pl.ds(2 * tok, 2 * HALO)]
            remote(spot, spot, halo_send, halo_recv, partner).wait_recv()

        for copy in maps:
            copy.wait()
        put(pbc, pl.ds(0, 2 * N), dot(xe[...], wbc[...]).astype(BF16).astype(F32))
        for s in range(2):
            bm[seq_rows(s), :] = conv(pbc, s, pl.ds(0, N), tb[...])
            cm[seq_rows(s), :] = conv(pbc, s, pl.ds(N, N), tc[...])
        for s in range(2):
            cb[s] = dot(cm[seq_rows(s), :], bm[seq_rows(s), :], ((1,), (1,)))
        for copy in late:
            copy.wait()
        skip_vals.append(pick(skip[...], 1))

    def far_x(cols):
        acc = px[:, cols]
        for o in range(1, n_x):
            acc = acc + dot(xe[:, chip_rows(o)], wx[chip_rows(o), cols])
        put(pcx, cols, acc.astype(BF16).astype(F32))
        for s in range(2):
            xs[seq_rows(s), cols] = conv(pcx, s, cols, tx[:, cols])

    def far_z(cols):
        acc = gz[:, cols]
        for o in range(1, n_x):
            acc = acc + dot(xe[main, chip_rows(o)], wz[chip_rows(o), cols])
        gz[:, cols] = silu(acc.astype(BF16).astype(F32))

    def chain_copy(s, p):
        pc = pair_cols(p)
        return remote(
            snd.at[s, :, pc], car.at[s, :, pc], c_send, c_recv.at[s, p],
            {"sp": jnp.minimum(z + 1, n_sp - 1)},
        )

    def step_pairs(cols):
        return range(cols.start // (2 * P_SIZE), (cols.start + cols.size) // (2 * P_SIZE))

    def local_state(cols):
        for s in range(2):
            for p in step_pairs(cols):
                pc = pair_cols(p)
                v = s * pairs + p
                part = (xs[seq_rows(s), pc].astype(F32) * spread(step, v, first_head)).astype(BF16)
                scl[seq_rows(s), pc] = part
                sc[seq_rows(s), pc] = (part.astype(F32) * spread(to_end, v, first_head)).astype(BF16)
            st[s, :, cols] = dot(bm[seq_rows(s), :], sc[seq_rows(s), cols], ((0,), (0,)))

        @pl.when(z == 0)
        def _():
            for s in range(2):
                car[s, :, cols] = jnp.zeros((N, cols.size), BF16)
                for p in step_pairs(cols):
                    pc = pair_cols(p)
                    snd[s, :, pc] = st[s, :, pc].astype(BF16)
                    chain_copy(s, p).start()

    def chain(cols):
        for s in range(2):
            for p in step_pairs(cols):
                chain_copy(s, p).wait_recv()

                @pl.when(z < n_sp - 1)
                def _(s=s, p=p):
                    pc = pair_cols(p)
                    v = s * pairs + p
                    total = spread(whole, v, first_row) * car[s, :, pc].astype(F32) + st[s, :, pc]
                    snd[s, :, pc] = total.astype(BF16)
                    chain_copy(s, p).start()

    def chain_slot(slot, cols):
        @pl.when(jnp.minimum(z, 3) == slot)
        def _():
            chain(cols)

    def inner(s, cols):
        for p in step_pairs(cols):
            pc = pair_cols(p)
            parts = []
            for v in (s * per_group + 2 * p, s * per_group + 2 * p + 1):
                gap = jnp.where(lower, cum[:, v : v + 1] - cum_t[v : v + 1, :], -jnp.inf)
                parts.append(dot((cb[s] * jnp.exp(gap)).astype(BF16), scl[seq_rows(s), pc]))
            bypass = spread(skip_vals[0], p, first_row) * xs[seq_rows(s), pc].astype(F32)
            y[seq_rows(s), pc] = jnp.where(first_head, parts[0], parts[1]) + bypass

    def step_cols(s):
        return pl.ds(steps[s][1] * steps[s][2], steps[s][2])

    dp_pair = (dp, xi * 2 + 1 - core)

    def seq_rows_of(mine):
        return pl.ds(pl.multiple_of((core if mine else 1 - core) * tok, 16), tok)

    def gate(j):
        cols = pl.ds(j * block, block)
        for s in range(2):
            reached = dot(cm[seq_rows(s), :], car[s, :, cols])
            for p in step_pairs(cols):
                pc = pair_cols(p)
                here = slice(p * 2 * P_SIZE - cols.start, (p + 1) * 2 * P_SIZE - cols.start)
                mixed = y[seq_rows(s), pc] + spread(reach, s * pairs + p, first_head) * reached[:, here]
                y[seq_rows(s), pc] = mixed.astype(BF16).astype(F32) * gz[seq_rows(s), pc]

    def finish(mine):
        gated = y[seq_rows_of(mine), :]
        square = jnp.sum(gated * gated, axis=1, keepdims=True)
        inv = lax.rsqrt(square * (1.0 / gw) + EPSILON)
        normed = (gated * inv * scale[...]).astype(BF16)
        if mine:
            nrm[:, own_cols] = normed
        else:
            nsn[...] = normed
            remote(nsn, nrm.at[:, own_cols], n_send, n_recv.at[0], partner).start()

    def half_k(d, cols, group_cols):
        first = pl.multiple_of(d * width + group_cols.start, 128)
        return dot(nrm[:, group_cols], wf[pl.ds(first, gw), cols])

    def out_a():
        own[2].wait()
        spot = wf.at[out_rows(dp_pair[1])]
        remote(spot, spot, p_send.at[3], p_recv.at[5], partner).wait_recv()
        for i, d in enumerate(dp_pair):
            for j in range(0, fw, tile):
                cols = pl.ds(j, tile)
                acc[i, :, cols] = half_k(d, cols, own_cols)

    def out_b():
        spot = nrm.at[:, other_cols]
        remote(nsn, spot, n_send, n_recv.at[0], partner).wait_recv()
        for i, d in enumerate(dp_pair):
            for j in range(0, fw, tile):
                cols = pl.ds(j, tile)
                whole_cols = pl.ds(pl.multiple_of(d * fw + j, 128), tile)
                out_ref[:, whole_cols] = (acc[i, :, cols] + half_k(d, cols, other_cols)).astype(BF16)

    def forward_copy(o, s):
        spot = wf.at[out_rows(owner_of(o) * 2 + core), step_cols(s)]
        return remote(spot, spot, f_send, f_recv.at[f_steps.index(s)], partner)

    def forward(s):
        rest(s)
        for o in range(1, n_x):
            forward_copy(o, s).start()

    def output(j):
        cols = pl.ds(j * tile, tile)
        for s in f_steps:
            if step_cols(s).start // tile == j:
                spot = wf.at[pl.ds(0, (n_x - 1) * width), step_cols(s)]
                remote(spot, spot, f_send, f_recv.at[f_steps.index(s)], partner).wait_recv()
        for o in range(1, n_x):
            for d in (core, 1 - core):
                owner = owner_of(o) * 2 + d
                whole_cols = pl.ds(pl.multiple_of(owner * fw + cols.start, 128), cols.size)
                out_ref[:, whole_cols] = dot(nrm[...], wf[out_rows(owner), cols]).astype(BF16)

    f_steps = [s for s in range(len(steps)) if steps[s][0] == 2]
    tile = min(256, fw)
    block = 256

    def run(name):
        if name == "nearz":
            near(1)
            tiles(gw, 256, near_z)
        elif name == "pbc":
            maps_task()
        elif name == "nearx":
            near(0)
            tiles(gw, 256, near_x)
        elif name == "finishp":
            finish(False)
        elif name == "finisho":
            finish(True)
        elif name == "outa":
            out_a()
        elif name == "outb":
            out_b()
        else:
            task, s = name
            if task == "seeds":
                seeds(s)
            elif task == "cross":
                cross(s)
            elif task in ("relay0", "relay1"):
                relay(s, int(task[-1]))
            elif task == "farx":
                rest(s)
                far_x(step_cols(s))
            elif task == "state":
                local_state(step_cols(s))
            elif task == "inner":
                for q in range(2):
                    inner(q, step_cols(s))
            elif task == "farz":
                rest(s)
                far_z(step_cols(s))
            elif task == "gate":
                gate(s)
            elif task == "fwd":
                forward(s)
            else:
                output(s)

    for n, name in enumerate(order):
        for level in (1, 2, 3):
            for s, at in slots[level]:
                if at == n:
                    chain_slot(level, step_cols(s))
        run(name)

    def sent_wait(send, rows):
        if rows:
            spot = wx.at[pl.ds(0, rows)]
            remote(spot, spot, send, n_recv.at[0], partner).wait_send()

    for copy in sends:
        copy.wait_send()
    sent_wait(p_send.at[3], 2 * rows_dev + width * fw // gw)
    sent_wait(y_send, sent["y"])
    for b in range(2):

        @pl.when(zb == b)
        def _(b=b):
            sent_wait(z_send, sent["z"] + b * sent["across"])
            if sent[0, b] == sent[1, b]:
                sent_wait(x_send, sent[0, b])
            else:
                for c in range(2):

                    @pl.when(core == c)
                    def _(c=c):
                        sent_wait(x_send, sent[c, b])

    remote(nsn, nsn, n_send, n_recv.at[0], partner).wait_send()
    spot = wf.at[pl.ds(0, (n_x - 1) * width)]
    remote(spot, spot, f_send, n_recv.at[0], partner).wait_send()

    @pl.when(z < n_sp - 1)
    def _():
        spot = xe.at[pl.ds(2 * tok, 2 * HALO)]
        remote(spot, spot, halo_send, halo_recv, partner).wait_send()
        remote(snd, snd, c_send, n_recv.at[0], partner).wait_send()


def shards(
    dims,
    mixer_source_array,
    source_projection,
    gating_projection,
    entry_mapping_projection,
    readout_mapping_projection,
    increment_projection,
    source_conv_taps,
    entry_mapping_taps,
    readout_mapping_taps,
    increment_offsets,
    channel_damping_rate,
    bypass_coefficients,
    stride_multiplier,
    added_log_damping,
    norm_scale_factor,
    final_projection,
):
    n_grp, n_sp, n_dp = dims
    n_x = n_dp // 2
    hidden = mixer_source_array[0]
    tok, model = hidden.shape
    width = source_projection.shape[1]
    gw = width // G
    heads = increment_projection.shape[1]
    fw = final_projection.shape[1]
    length = stride_multiplier.shape[1]
    out_width = fw * n_dp
    steps, types, across = plan(n_sp, n_x, gw, fw)[:3]
    n_relay = sum(4 - kind for kind in types) + sum(across)
    n_steps = len(steps)
    n_far = sum(1 for step in steps if step[0] == 2)
    span = HALO + tok
    dma = pltpu.SemaphoreType.DMA
    hbm = pl.BlockSpec(memory_space=pl.ANY)
    output = pl.pallas_call(
        functools.partial(kernel, dims),
        out_shape=pltpu.VMEM((tok, out_width), BF16),
        in_specs=[hbm] * 16,
        out_specs=pl.BlockSpec(memory_space=pltpu.VMEM),
        scratch_shapes=[
            pltpu.VMEM((2 * span, model), BF16),
            pltpu.VMEM((model, gw), BF16),
            pltpu.VMEM((model, gw), BF16),
            pltpu.VMEM((n_dp * width, fw), BF16),
            pltpu.VMEM((model, 2 * N), BF16),
            pltpu.VMEM((heads, model), BF16),
            pltpu.VMEM((CONV_W, gw), F32),
            pltpu.VMEM((CONV_W, N), F32),
            pltpu.VMEM((CONV_W, N), F32),
            pltpu.VMEM((1, heads), F32),
            pltpu.VMEM((1, heads), F32),
            pltpu.VMEM((1, heads), F32),
            pltpu.VMEM((2, 1, length), F32),
            pltpu.VMEM((2, heads // G, length), F32),
            pltpu.VMEM((1, gw), F32),
            pltpu.VMEM((2 * span, 2 * N), F32),
            pltpu.VMEM((2 * span, gw), F32),
            pltpu.VMEM((2 * span, gw), F32),
            pltpu.VMEM((2 * tok, gw), F32),
            pltpu.VMEM((2 * tok, N), BF16),
            pltpu.VMEM((2 * tok, N), BF16),
            pltpu.VMEM((2, tok, tok), F32),
            pltpu.VMEM((2 * tok, gw), BF16),
            pltpu.VMEM((2 * tok, gw), BF16),
            pltpu.VMEM((2 * tok, gw), BF16),
            pltpu.VMEM((2 * tok, gw), F32),
            pltpu.VMEM((2, N, gw), F32),
            pltpu.VMEM((2, N, gw), BF16),
            pltpu.VMEM((2, N, gw), BF16),
            pltpu.VMEM((tok, width), BF16),
            pltpu.VMEM((tok, gw), BF16),
            pltpu.VMEM((2, tok, fw), F32),
            dma((16,)),
            dma((4,)),
            dma((7,)),
            dma((7,)),
            dma((n_steps,)),
            dma((n_steps,)),
            dma((max(n_relay, 1),)),
            dma((2, heads // G // 2)),
            dma((1,)),
            dma((n_far,)),
        ],
        compiler_params=pltpu.CompilerParams(
            collective_id=0, has_side_effects=True, vmem_limit_bytes=56 * 1024 * 1024
        ),
    )(
        hidden,
        source_projection,
        gating_projection,
        final_projection,
        entry_mapping_projection,
        readout_mapping_projection,
        increment_projection.T,
        source_conv_taps,
        entry_mapping_taps,
        readout_mapping_taps,
        increment_offsets[None],
        channel_damping_rate[None],
        bypass_coefficients[None],
        stride_multiplier,
        jnp.swapaxes(added_log_damping, 1, 2),
        norm_scale_factor[None],
    )
    return output[None]


def solution(mesh):
    n_grp, n_sp, n_dp = (mesh.shape[a] for a in ("grp", "sp", "dp"))
    return jax.shard_map(
        functools.partial(shards, (n_grp, n_sp, n_dp)),
        mesh=mesh,
        in_specs=(
            P(("grp", "dp"), "sp", None),
            P("dp", None),
            P("dp", None),
            P(),
            P(),
            P(),
            P(),
            P(),
            P(),
            P(),
            P(),
            P(),
            P(("grp", "dp"), None),
            P(("grp", "dp"), None, None),
            P(),
            P(None, "dp"),
        ),
        out_specs=P(("grp", "dp"), "sp", None),
        check_vma=False,
    )
```
